32 devices in a mesh: sp: 8 (over z, y), tp: 4 (over x, core).
Axes of the slice: x: 2, y: 2, z: 4, core: 2. Of those that a mesh axis runs over, the one named last changes fastest.
Arguments:
- tokens: bfloat16 [4, 3072, 2048], P(None, 'sp'), may hold values from -21 to 21
- query_weight: bfloat16 [2048, 1024], P(None, 'tp'), may hold values from -0.125 to 0.125
- key_weight: bfloat16 [2048, 1024], P(None, 'tp'), may hold values from -0.125 to 0.125
- value_weight: bfloat16 [2048, 1024], P(None, 'tp'), may hold values from -0.125 to 0.125
- out_gain: float32 [1024], replicated, may hold values from 0.1 to 1.9
- out_weight: bfloat16 [1024, 2048], P(None, 'tp'), may hold values from -0.1875 to 0.1875
Outputs:
- mixed_out: bfloat16 [4, 3072, 2048], P(None, 'sp', 'tp')
- total_log: float32 [4, 8, 3072], P(None, 'tp', 'sp')
The draws below stay inside these ranges and needn't reach their ends.
All inputs are finite; a program needn't handle non-finite values.
Results may differ from the reference program's by a relative error of at most 0.0098.
Values may be sent and summed in bfloat16 or wider, within the bound.
A program may use at most 128 MiB of HBM per device.

```python
import jax
import jax.numpy as jnp
from jax import lax

D = 2048
HEADS = 8
HEAD_DIM = 128
REACH = 64
SEQS = 4
TOK_DEV = 384
TOKENS = 3072


def draw_tokens(key, part):
    dims = (SEQS, TOKENS, D)
    return jnp.clip(jax.random.normal(key, dims, jnp.float32), -6.0, 6.0).astype(jnp.bfloat16)


def block_levels(rng, shape, cuts, least, high):
    factor_of, own = 1.0, jax.random.fold_in(rng, 6)
    for axis_at, blocks in cuts:
        heights = jnp.exp(jax.random.uniform(jax.random.fold_in(own, axis_at), (blocks,), jnp.float32, least / len(cuts), high / len(cuts)))
        factor_of = factor_of * jnp.repeat(heights, shape[axis_at] // blocks).reshape([-1 if axis == axis_at else 1 for axis in range(len(shape))])
    return factor_of


def bell_draw(rng, shape, deviation, bound, cuts=(), kind=jnp.bfloat16):
    entries = jax.random.normal(rng, shape, jnp.float32) * deviation
    if len(cuts) > 0:
        entries = block_levels(rng, shape, cuts, -0.22, 0.18) * entries
    return jnp.clip(entries, min=-bound, max=bound).astype(kind)


def setup_inputs(seed: int = 0) -> dict:
    arg_keys = jax.random.split(jax.random.key(seed), 7)
    tokens = draw_tokens(jax.random.fold_in(arg_keys[6], 71), 0)
    query_weight = bell_draw(arg_keys[1], (D, HEADS * HEAD_DIM), D ** -0.5, 0.125, ((1, 4),))
    key_weight = bell_draw(arg_keys[2], (D, HEADS * HEAD_DIM), D ** -0.5, 0.125, ((1, 4),))
    value_weight = bell_draw(arg_keys[3], (D, HEADS * HEAD_DIM), D ** -0.5, 0.125, ((1, 4),))
    out_gain = jnp.clip(1.0 + 0.18 * jax.random.normal(arg_keys[4], (HEADS * HEAD_DIM,), jnp.float32), 0.1, 1.9)
    out_weight = bell_draw(arg_keys[5], (HEADS * HEAD_DIM, D), (HEADS * HEAD_DIM) ** -0.5, 0.1875, ((1, 4),))
    return {"tokens": tokens, "query_weight": query_weight, "key_weight": key_weight, "value_weight": value_weight, "out_gain": out_gain, "out_weight": out_weight}


DILATIONS = (1, 4, 16)
ROPE_BASE = 10000.0
MASK_FILL = -1e+30
NORM_FLOOR = 1e-06

def rotate(projected, positions):
    in_shape = projected.shape
    heads_view = projected.reshape(in_shape[0], in_shape[1], -1, HEAD_DIM)
    half_dim = HEAD_DIM // 2
    frequency = ROPE_BASE ** (-jnp.arange(half_dim, dtype=jnp.float32) / half_dim)
    angles = positions.astype(jnp.float32)[:, None] * frequency[None, :]
    cosine = jnp.cos(angles)[None, :, None, :]
    sine_part = jnp.sin(angles)[None, :, None, :]
    lower_half = heads_view[..., :half_dim]
    upper_half = heads_view[..., half_dim:]
    turned = jnp.concatenate([lower_half * cosine - upper_half * sine_part, upper_half * cosine + lower_half * sine_part], axis=-1)
    return turned.reshape(in_shape)

def band_attend(queries, extended, dilation, offset, total_len):
    seq_count, length, channels = queries.shape
    head_count = channels // HEAD_DIM
    reach_span = REACH * dilation
    query_rows = length // dilation
    key_rows = query_rows + 2 * REACH
    shaped_q = queries.reshape(seq_count, query_rows, dilation, head_count, HEAD_DIM).astype(jnp.float32)
    shaped_k = extended[:, :, :channels].reshape(seq_count, key_rows, dilation, head_count, HEAD_DIM).astype(jnp.float32)
    shaped_v = extended[:, :, channels:].reshape(seq_count, key_rows, dilation, head_count, HEAD_DIM).astype(jnp.float32)
    scores = jnp.einsum('sarhe,sbrhe->srhab', shaped_q, shaped_k)
    query_row = jnp.arange(query_rows, dtype=jnp.int32)[:, None]
    key_row = jnp.arange(key_rows, dtype=jnp.int32)[None, :]
    inband = (key_row >= query_row) & (key_row <= query_row + 2 * REACH)
    residue = jnp.arange(dilation, dtype=jnp.int32)[:, None, None]
    key_pos = offset - reach_span + key_row[None] * dilation + residue
    allowed = inband[None] & (key_pos >= 0) & (key_pos < total_len)
    scores = jnp.where(allowed[None, :, None], scores * HEAD_DIM ** (-0.5), MASK_FILL)
    maximum = lax.optimization_barrier(jnp.max(scores, axis=-1, keepdims=True))
    exp_scores = jnp.exp(scores - maximum)
    weight_sum = lax.optimization_barrier(jnp.sum(exp_scores, axis=-1, keepdims=True))
    probs = lax.optimization_barrier(exp_scores.astype(jnp.bfloat16)).astype(jnp.float32)
    branch = jnp.einsum('srhab,sbrhe->sarhe', probs, shaped_v)
    branch = branch / jnp.transpose(weight_sum, (0, 3, 1, 2, 4))
    branch = branch.reshape(seq_count, length, head_count, HEAD_DIM)
    log_sum = (maximum + jnp.log(weight_sum))[..., 0]
    log_sum = jnp.transpose(log_sum, (0, 2, 3, 1)).reshape(seq_count, head_count, length)
    return (branch, log_sum)

def combine(branch_out, branch_log):
    logs = jnp.stack(branch_log, 0)
    peak = lax.optimization_barrier(jnp.max(logs, axis=0))
    total_log = peak + jnp.log(lax.optimization_barrier(jnp.sum(jnp.exp(logs - peak[None]), axis=0)))
    shares = jnp.exp(logs - total_log[None])
    shares = jnp.transpose(shares, (0, 1, 3, 2))[..., None]
    merged = lax.optimization_barrier(jnp.sum(shares * jnp.stack(branch_out, 0), axis=0))
    seq_count, length, head_count, head_dim = merged.shape
    return (merged.reshape(seq_count, length, head_count * head_dim).astype(jnp.bfloat16), total_log)

def reference(tokens, query_weight, key_weight, value_weight, out_gain, out_weight):
    flat_rows = tokens.reshape(SEQS * TOKENS, D)
    positions = jnp.arange(TOKENS, dtype=jnp.int32)

    def project(weight):
        return jnp.dot(flat_rows, weight, preferred_element_type=jnp.float32).reshape(SEQS, TOKENS, -1)
    queries = rotate(project(query_weight), positions).astype(jnp.bfloat16)
    key_rows = rotate(project(key_weight), positions).astype(jnp.bfloat16)
    values = project(value_weight).astype(jnp.bfloat16)
    wide_span = REACH * DILATIONS[2]
    stacked = jnp.pad(jnp.concatenate([key_rows, values], axis=2), ((0, 0), (wide_span, wide_span), (0, 0)))

    def one_block(block_index):
        row_start = (block_index * TOK_DEV).astype(jnp.int32)
        block_q = lax.dynamic_slice_in_dim(queries, row_start, TOK_DEV, 1)
        branch_out = []
        branch_log = []
        for dilation in DILATIONS:
            reach_span = REACH * dilation
            extended = lax.dynamic_slice_in_dim(stacked, row_start + wide_span - reach_span, TOK_DEV + 2 * reach_span, 1)
            branch, log_sum = band_attend(block_q, extended, dilation, row_start, TOKENS)
            branch_out.append(branch)
            branch_log.append(log_sum)
        return combine(branch_out, branch_log)
    merged, total_log = lax.map(one_block, jnp.arange(TOKENS // TOK_DEV, dtype=jnp.int32))
    merged = jnp.transpose(merged, (1, 0, 2, 3)).reshape(SEQS, TOKENS, HEADS * HEAD_DIM)
    total_log = jnp.transpose(total_log, (1, 2, 0, 3)).reshape(SEQS, HEADS, TOKENS)
    lifted = merged.astype(jnp.float32)
    square = lax.optimization_barrier(jnp.mean(lifted * lifted, axis=-1))
    scaled = (lifted * out_gain.astype(jnp.float32)).astype(jnp.bfloat16)
    projected = jnp.dot(scaled.reshape(SEQS * TOKENS, HEADS * HEAD_DIM), out_weight, preferred_element_type=jnp.float32).reshape(SEQS, TOKENS, D)
    mixed_out = (projected * lax.rsqrt(square + NORM_FLOOR)[..., None]).astype(jnp.bfloat16)
    return (mixed_out, total_log)
```

```python
import functools
import math

import jax
import jax.numpy as jnp
import numpy as np
from jax import lax
from jax.experimental import pallas as pl
from jax.experimental.pallas import tpu as pltpu
from jax.sharding import PartitionSpec as P

HEAD_DIM = 128
REACH = 64
FAR = 16
NEAR = 4
GRAN = FAR * FAR
ROPE_BASE = 10000.0
MASK_FILL = -1e30
NORM_FLOOR = 1e-06
LOG2E = 1.0 / math.log(2.0)
LN2 = math.log(2.0)
F32 = jnp.float32
BF16 = jnp.bfloat16

MESH = pl.DeviceIdType.MESH


def iota(shape, dim):
    return lax.broadcasted_iota(jnp.int32, shape, dim)


def perm_token(p):
    slot = p // FAR
    a = p % FAR
    residue = slot // NEAR + NEAR * (slot % (FAR // NEAR))
    return a * FAR + residue


def dot_t(a, b):
    return lax.dot_general(a, b, (((1,), (1,)), ((), ())), preferred_element_type=F32)


def layer_kernel(
    nsp, tok_h, wq_h, wk_h, wv_h, wo_h, cos_h, sin_h, cos_base_h, sin_base_h, gain_h,
    out, log_out,
    tok, wq, wk, wv, wo, cos, sin, cos_base, sin_base, gain, kn, qn, kvs, qs, gath, outs, logs,
    lsend, lrow, kp, qp, on, perm, unperm, bias1, bias4, bias16, bias_end, o1, m1, l1,
    load_sem, send_sem, recv_sem,
):
    half = tok.shape[0] // 2
    units = kn.shape[0]
    length = tok.shape[1]
    block = 2 * length
    grans = block // GRAN
    wide = REACH * FAR
    side = wide // GRAN
    tail = wide - block
    span = block + 2 * wide
    rows = block // FAR
    ends = tail // GRAN
    key_rows = (span - 2 * tail) // FAR
    near_rows = rows + 2 * FAR
    cols = wq.shape[1]
    heads = cols // HEAD_DIM
    total = nsp * length
    scale = HEAD_DIM**-0.5 * LOG2E
    sp, t = lax.axis_index("sp"), lax.axis_index("tp")
    y, blk = sp % 2, sp // 2
    twin = sp + 1 - 2 * y
    x_peer = (t + 2) % 4
    d_peer = t + 1 - 2 * (t % 2)
    x_d_peer = (d_peer + 2) % 4
    mine, other = y * half, (1 - y) * half

    loads = []

    def load(src, dst):
        copy = pltpu.make_async_copy(src, dst, load_sem.at[len(loads)])
        copy.start()
        loads.append(copy)
        return copy

    got_tables = [
        load(*pair)
        for pair in (
            (cos_base_h, cos_base), (sin_base_h, sin_base), (cos_h, cos), (sin_h, sin)
        )
    ]
    cuts = (pl.ds(0, length // 3), pl.ds(length // 3, length - length // 3))
    got_wk, got_wv = load(wk_h, wk), load(wv_h, wv)
    got_first = [load(tok_h.at[mine, cut], tok.at[0, cut]) for cut in cuts]
    got_tok = {}

    barrier = pltpu.get_barrier_semaphore()
    has = {d: (sp + d >= 0) & (sp + d < nsp) for d in (2, -2, 4, -4)}
    reach = {d: has[d] & has[-d] for d in (2, -2)}
    for peer in ((twin, t), (sp, x_peer), (sp, d_peer)):
        pl.semaphore_signal(barrier, inc=1, device_id=peer, device_id_type=MESH)
    count = 3
    for d in (2, -2):
        there = has[d]
        count = count + there.astype(jnp.int32)

        @pl.when(there)
        def _(d=d):
            pl.semaphore_signal(barrier, inc=1, device_id=(sp + d, t), device_id_type=MESH)

    first = pl.multiple_of(y * length, HEAD_DIM)
    second = pl.multiple_of((1 - y) * length, HEAD_DIM)

    def clear(d, at, size):
        @pl.when(jnp.logical_not(has[d]))
        def _():
            for u in range(units):
                kn[u, at : at + size] = jnp.zeros((size, kn.shape[2]), BF16)

    numbers = {}

    def copy(name, src, dst, peer):
        n = numbers.setdefault(name, len(numbers))
        return pltpu.make_async_remote_copy(
            src_ref=src, dst_ref=dst, send_sem=send_sem.at[n], recv_sem=recv_sem.at[n],
            device_id=peer, device_id_type=MESH,
        )

    sent = []

    def start(c):
        c.start()
        sent.append((c, None))

    def z_copy(kind, u, d, cut=None):
        if kind == "T":
            src = wide - tail if d > 0 else wide + block
            dst = 0 if d > 0 else span - tail
            size = tail
        else:
            if kind == "S":
                at, size = block - tail if d > 0 else 0, tail
            elif kind == "R":
                at, size = 0 if d > 0 else tail, block - tail
            else:
                at, size = first if kind == "A" else second, length
            if cut is not None:
                at, size = at + cut.start, cut.size
            src = wide + at
            dst = (tail if d > 0 else wide + block) + at
        return copy(
            (kind, u, d, cut and cut.start), kn.at[u, pl.ds(src, size)], kn.at[u, pl.ds(dst, size)],
            (sp + d, t),
        )

    def z_start(kind, u, cut=None):
        for d in (2, -2):
            c = z_copy(kind, u, d, cut)
            there = reach[d] if kind == "T" else has[d]

            @pl.when(there)
            def _():
                c.start()

            sent.append((c, there))

    def z_wait(kind, u):
        for d in (2, -2):

            @pl.when(has[-2 * d] if kind == "T" else has[-d])
            def _():
                for cut in cuts if kind == "A" and u < heads else (None,):
                    z_copy(kind, u, d, cut).wait_recv()

    every = pl.ds(0, length)

    def turned(x, w, store, cut=every):
        a = jnp.dot(x, w[...], preferred_element_type=F32)
        for h in range(heads):
            one = a[:, h * HEAD_DIM : (h + 1) * HEAD_DIM]
            other_half = pltpu.roll(one, HEAD_DIM // 2, 1)
            store(h, (one * cos[cut] + other_half * sin[cut]).astype(BF16))

    def lanes(n):
        return slice(n * HEAD_DIM, (n + 1) * HEAD_DIM)

    def keys_values(x, put, cut=every):
        turned(x, wk, lambda h, a: put(2 * h, a), cut)
        v = jnp.dot(x, wv[...], preferred_element_type=F32).astype(BF16)
        for h in range(heads):
            put(2 * h + 1, v[:, lanes(h)])

    def own_kv(s, cut=every):
        def put(n, a):
            at = pl.ds(wide + first + cut.start, cut.size)
            kn[s * heads + n // 2, at, lanes(n % 2)] = a

        keys_values(tok[2 * s, cut], put, cut)

    def twin_kv(s):
        def put(n, a):
            kvs[s * heads + n // 2, :, lanes(n % 2)] = a

        keys_values(tok[2 * s + 1], put)

    def own_q(s):
        def put(n, a):
            qn[s * heads + n, pl.ds(first, length)] = a

        turned(tok[2 * s], wq, put)

    def twin_q(s):
        def put(n, a):
            qs[s * heads + n] = a

        turned(tok[2 * s + 1], wq, put)

    def y_kv(u, at):
        return copy(("yk", u), kvs.at[u], kn.at[u, pl.ds(wide + at, length)], (twin, t))

    def y_q(u, at):
        return copy(("yq", u), qs.at[u], qn.at[u, pl.ds(at, length)], (twin, t))

    def of(s):
        return range(s * heads, (s + 1) * heads)

    for c in got_tables:
        c.wait()
    cos_at, sin_at = cos_base[pl.ds(sp, 1)], sin_base[pl.ds(sp, 1)]
    sign = jnp.where(iota(cos.shape, 1) < HEAD_DIM // 2, -1.0, 1.0)
    cos_step, sin_step = cos[...], sin[...]
    cos[...] = cos_step * cos_at - sin_step * sin_at
    sin[...] = (sin_step * cos_at + cos_step * sin_at) * sign
    for c in (got_wk, got_wv, got_first[0]):
        c.wait()
    got_tok["o", 0] = load(tok_h.at[other], tok.at[1])
    own_kv(0, cuts[0])
    pl.semaphore_wait(barrier, count)
    for u in of(0):
        z_start("A", u, cuts[0])
    got_wq = load(wq_h, wq)
    got_first[1].wait()
    own_kv(0, cuts[1])
    for u in of(0):
        z_start("A", u, cuts[1])
    got_tok["o", 0].wait()
    for s in range(1, half):
        got_tok["o", s] = load(tok_h.at[other + s], tok.at[2 * s + 1])
        got_tok["m", s] = load(tok_h.at[mine + s], tok.at[2 * s])
    got_gain = load(gain_h, gain)
    got_wo = load(wo_h, wo)
    twin_kv(0)
    for u in of(0):
        start(y_kv(u, first))
    got_wq.wait()
    twin_q(0)
    for u in of(0):
        start(y_q(u, first))
    for s in range(1, half):
        got_tok["o", s].wait()
        got_tok["m", s].wait()
        twin_kv(s)
        for u in of(s):
            start(y_kv(u, first))
        own_kv(s)
        twin_q(s)
        for u in of(s):
            start(y_q(u, first))
    y_kv(0, second).wait_recv()
    z_start("B", 0)
    own_q(0)

    clear(-4, 0, tail)
    clear(-2, tail, block)
    clear(2, wide + block, block)
    clear(4, span - tail, tail)
    perm[...] = jnp.where(
        iota((GRAN, GRAN), 1) == perm_token(iota((GRAN, GRAN), 0)), 1.0, 0.0
    ).astype(BF16)
    unperm[...] = jnp.where(
        iota((GRAN, GRAN), 0) == perm_token(iota((GRAN, GRAN), 1)), 1.0, 0.0
    ).astype(BF16)
    origin = blk * block - wide
    shape = (GRAN, GRAN + 2 * REACH)
    token = perm_token(iota(shape, 0))
    for g in range(grans):
        q_at = wide + g * GRAN + token
        k_at = wide + g * GRAN - REACH + iota(shape, 1)
        ok = (jnp.abs(k_at - q_at) <= REACH) & (k_at + origin >= 0) & (k_at + origin < total)
        bias1[g] = jnp.where(ok, 0.0, MASK_FILL)
    per = FAR // NEAR
    shape = (per * rows, per * near_rows)
    row, col = iota(shape, 0), iota(shape, 1)
    q_at = (row % rows + side * FAR) * FAR + NEAR * (row // rows)
    k_at = (col % near_rows + (side - 1) * FAR) * FAR + NEAR * (col // near_rows)
    ok = (jnp.abs(k_at - q_at) <= REACH * NEAR) & (k_at + origin >= 0) & (k_at + origin < total)
    bias4[...] = jnp.where(ok, 0.0, MASK_FILL)
    shape = (rows, key_rows)
    q_at = iota(shape, 0) + side * FAR
    k_at = iota(shape, 1) + ends * FAR
    ok = (
        (jnp.abs(k_at - q_at) <= REACH)
        & (k_at * FAR + origin >= 0)
        & (k_at * FAR + origin < total)
    )
    bias16[...] = jnp.where(ok, 0.0, MASK_FILL)
    reached = [(g, 0) for g in range(ends)]
    reached += [(g, span - tail) for g in range(grans - ends, grans)]
    shape = (GRAN, tail)
    token = perm_token(iota(shape, 0))
    for n, (g, at) in enumerate(reached):
        gap = at + iota(shape, 1) - (wide + g * GRAN + token)
        k_at = at + iota(shape, 1) + origin
        ok = (gap % FAR == 0) & (jnp.abs(gap) <= wide) & (k_at >= 0) & (k_at < total)
        bias_end[n] = jnp.where(ok, 0.0, MASK_FILL)

    y_kv(1, second).wait_recv()
    z_start("B", 1)
    for s in range(1, half):
        own_q(s)

    near_from, near_to = side - 1, side + grans + 1

    def gather_keys(u, slot, chunks):
        for j in chunks:
            moved = jnp.dot(
                perm[...], kn[u, j * GRAN : (j + 1) * GRAN], preferred_element_type=F32
            )
            moved = moved.astype(BF16).reshape(FAR, FAR, 2 * HEAD_DIM)
            at = (j - ends) * FAR
            kp[slot, :, at : at + FAR] = moved

    flat = (per * rows, HEAD_DIM)
    cube = (per, rows, HEAD_DIM)

    def merge(slot, sel, scores, weigh):
        m_old = m1[slot, sel].reshape(flat)
        m_new = jnp.maximum(m_old, jnp.max(scores, axis=1, keepdims=True))
        keep = jnp.exp2(m_old - m_new)
        p = jnp.exp2(scores - m_new[:, :1])
        l = l1[slot, sel].reshape(flat) * keep + jnp.sum(p, axis=1, keepdims=True)
        o = o1[slot, sel].reshape(flat) * keep + weigh(p.astype(BF16))
        for ref, a in ((o1, o), (m1, m_new), (l1, l)):
            ref[slot, sel] = a.reshape(cube)

    def attend_near(u):
        slot = u % 2
        y_q(u, second).wait_recv()
        gather_keys(u, slot, range(near_from, near_to))
        for g in range(grans):
            moved = jnp.dot(
                perm[...], qn[u, g * GRAN : (g + 1) * GRAN], preferred_element_type=F32
            )
            moved = moved.astype(BF16)
            qp[slot, :, g * FAR : (g + 1) * FAR] = moved.reshape(FAR, FAR, HEAD_DIM)
            at = wide + g * GRAN - REACH
            k = kn[u, at : at + GRAN + 2 * REACH, :HEAD_DIM]
            v = kn[u, at : at + GRAN + 2 * REACH, HEAD_DIM:]
            sc = dot_t(moved, k) * scale + bias1[g]
            m = jnp.max(sc, axis=1, keepdims=True)
            p = jnp.exp2(sc - m)
            l = jnp.sum(p, axis=1, keepdims=True)
            o = jnp.dot(p.astype(BF16), v, preferred_element_type=F32)
            cut = (FAR, FAR, HEAD_DIM)
            o1[slot, :, g * FAR : (g + 1) * FAR] = o.reshape(cut)
            m1[slot, :, g * FAR : (g + 1) * FAR] = jnp.broadcast_to(m, o.shape).reshape(cut)
            l1[slot, :, g * FAR : (g + 1) * FAR] = jnp.broadcast_to(l, o.shape).reshape(cut)

        near_at = (near_from - ends) * FAR
        for group in range(NEAR):
            sel = slice(group * per, (group + 1) * per)
            k4 = kp[slot, sel, near_at : near_at + near_rows, :HEAD_DIM].reshape(-1, HEAD_DIM)
            v4 = kp[slot, sel, near_at : near_at + near_rows, HEAD_DIM:].reshape(-1, HEAD_DIM)
            s4 = dot_t(qp[slot, sel].reshape(flat), k4) * scale + bias4[...]
            merge(slot, sel, s4, lambda p: jnp.dot(p, v4, preferred_element_type=F32))

    def attend_far(u):
        slot = u % 2
        gather_keys(u, slot, [*range(ends, near_from), *range(near_to, span // GRAN - ends)])
        for group in range(NEAR):
            sel = slice(group * per, (group + 1) * per)
            own = range(group * per, (group + 1) * per)
            b16 = bias16[...]
            s16 = [dot_t(qp[slot, r], kp[slot, r, :, :HEAD_DIM]) * scale + b16 for r in own]

            def weigh(p):
                return jnp.concatenate(
                    [
                        jnp.dot(
                            p[i * rows : (i + 1) * rows], kp[slot, r, :, HEAD_DIM:],
                            preferred_element_type=F32,
                        )
                        for i, r in enumerate(own)
                    ],
                    axis=0,
                )

            merge(slot, sel, jnp.concatenate(s16, axis=0), weigh)
        for g in range(ends, grans - ends):
            settle(slot, g, *state(slot, g))

    def state(slot, g):
        cut = slice(g * FAR, (g + 1) * FAR)
        return [ref[slot, :, cut].reshape(GRAN, HEAD_DIM) for ref in (o1, m1, l1)]

    def settle(slot, g, o, m, l):
        merged = jnp.dot(unperm[...], (o / l).astype(BF16), preferred_element_type=F32)
        on[slot, g * GRAN : (g + 1) * GRAN] = merged.astype(BF16)
        x = m * LN2 + jnp.log(l)
        high = x.astype(BF16).astype(F32)
        mid = (x - high).astype(BF16).astype(F32)
        low = x - high - mid
        lane = iota((GRAN, HEAD_DIM), 1)
        terms = jnp.where(
            lane == 0, high, jnp.where(lane == 1, mid, jnp.where(lane == 2, low, 0.0))
        )
        pick = jnp.where(iota((FAR, HEAD_DIM), 0) == iota((FAR, HEAD_DIM), 1), 1.0, 0.0)
        turned_terms = dot_t(pick.astype(BF16), terms.astype(BF16)).astype(BF16)
        placed = jnp.dot(turned_terms, perm[...], preferred_element_type=F32)
        lrow[slot, :, g * GRAN : (g + 1) * GRAN] = jnp.sum(placed, axis=0, keepdims=True)

    def attend_end(u):
        slot = u % 2
        z_wait("T", u)
        for n, (g, at) in enumerate(reached):
            o_old, m_old, l_old = state(slot, g)
            q = qp[slot, :, g * FAR : (g + 1) * FAR].reshape(GRAN, HEAD_DIM)
            k = kn[u, at : at + tail, :HEAD_DIM]
            v = kn[u, at : at + tail, HEAD_DIM:]
            sc = dot_t(q, k) * scale + bias_end[n]
            m = jnp.maximum(m_old, jnp.max(sc, axis=1, keepdims=True))
            keep = jnp.exp2(m_old - m)
            p = jnp.exp2(sc - m[:, :1])
            l = l_old * keep + jnp.sum(p, axis=1, keepdims=True)
            o = o_old * keep + jnp.dot(p.astype(BF16), v, preferred_element_type=F32)
            settle(slot, g, o, m, l)

    def some(part, half_at):
        if part is None:
            return every
        at = (1 - half_at) * tail if part == "mid" else half_at * (length - tail)
        size = length - tail if part == "mid" else tail
        return pl.ds(pl.multiple_of(at, HEAD_DIM), size)

    def across(u, base, half_at, part):
        cut = some(part, half_at)
        return copy(
            ("yo", u, part), outs.at[u, cut], gath.at[t, base + u // heads, u % heads, cut],
            (twin, t),
        )

    def log_across(u, base):
        return copy(("yl", u), lsend.at[u], logs.at[base + u // heads, u % heads], (twin, t))

    def piece(name, u, owner, base, peer, part):
        ref = gath.at[owner, base + u // heads, u % heads, some(part, y)]
        return copy((name, u, part), ref, ref, peer)

    def publish(u, part=None):
        slot = u % 2
        s, h = u // heads, u % heads

        def put(ref, half_at):
            cut = some(part, half_at)
            at = pl.multiple_of(half_at * length + cut.start, HEAD_DIM)
            ref[cut] = on[slot, pl.ds(at, cut.size)]

        put(outs.at[u], 1 - y)
        start(across(u, mine, 1 - y, part))
        put(gath.at[t, mine + s, h], y)
        start(piece("xm", u, t, mine, (sp, x_peer), part))
        start(piece("dm", u, t, mine, (sp, d_peer), part))
        if part != "mid":
            logs[mine + s, h] = lrow[slot, :, pl.ds(first, length)]
            lsend[u] = lrow[slot, :, pl.ds(second, length)]
            start(log_across(u, mine))

    def spread(u, part=None):
        across(u, other, y, part).wait_recv()
        start(piece("xr", u, t, other, (sp, x_peer), part))
        start(piece("dr", u, t, other, (sp, d_peer), part))
        piece("xm", u, x_peer, mine, (sp, x_peer), part).wait_recv()
        start(piece("em", u, x_peer, mine, (sp, d_peer), part))

    def spread_twin(u, part=None):
        piece("xr", u, x_peer, other, (sp, x_peer), part).wait_recv()
        start(piece("er", u, x_peer, other, (sp, d_peer), part))
        if part != "mid":
            log_across(u, other).wait_recv()

    def finish(j):
        acc = None
        square = None
        for n in range(gath.shape[0]):
            x = jnp.concatenate([gath[n, j, h] for h in range(heads)], axis=1).astype(F32)
            at = slice(n * cols, (n + 1) * cols)
            scaled = (x * gain[:, at]).astype(BF16)
            term = jnp.dot(scaled, wo[at], preferred_element_type=F32)
            sq = jnp.sum(x * x, axis=1, keepdims=True)
            acc = term if acc is None else acc + term
            square = sq if square is None else square + sq
        out[j] = (acc * lax.rsqrt(square / wo.shape[0] + NORM_FLOOR)).astype(BF16)

    def parts_of(u):
        return ("mid", "end") if u == units - 1 else (None,)

    def finish_mine(s):
        for u in of(s):
            for part in parts_of(u):
                piece("dm", u, d_peer, mine, (sp, d_peer), part).wait_recv()
                piece("em", u, x_d_peer, mine, (sp, d_peer), part).wait_recv()
        finish(mine + s)

    def finish_other(s):
        for u in of(s):
            for part in parts_of(u):
                piece("dr", u, d_peer, other, (sp, d_peer), part).wait_recv()
                piece("er", u, x_d_peer, other, (sp, d_peer), part).wait_recv()
        finish(other + s)

    def arrived(u):
        z_wait("A", u)
        z_wait("B", u)

    arrived(0)
    z_start("T", 0)
    z_start("A", 2)
    attend_near(0)
    attend_far(0)
    arrived(1)
    z_start("T", 1)
    attend_near(1)
    y_kv(2, second).wait_recv()
    z_start("B", 2)
    attend_end(0)
    publish(0)
    attend_far(1)
    y_kv(3, second).wait_recv()
    z_start("S", 3)
    attend_end(1)
    publish(1)
    arrived(2)
    z_start("T", 2)
    z_start("R", 3)
    attend_near(2)
    attend_far(2)
    z_wait("S", 3)
    z_start("T", 3)
    spread(0)
    spread(1)
    attend_near(3)
    attend_end(2)
    publish(2)
    spread_twin(0)
    got_gain.wait()
    got_wo.wait()
    finish_mine(0)
    spread_twin(1)
    finish_other(0)
    spread(2)
    z_wait("R", 3)
    attend_far(3)
    publish(3, "mid")
    attend_end(3)
    publish(3, "end")
    spread_twin(2)
    spread(3, "mid")
    spread(3, "end")
    spread_twin(3, "mid")
    finish_mine(1)
    spread_twin(3, "end")
    finish_other(1)
    for j in range(logs.shape[0]):
        for h in range(heads):
            log_out[j, h : h + 1] = logs[j, h]
    for c, there in sent:
        if there is None:
            c.wait_send()
        else:

            @pl.when(there)
            def _(c=c):
                c.wait_send()


def layer(nsp, ntp, tokens, wq, wk, wv, wo, tables, gain):
    seqs, length, width = tokens.shape
    half = seqs // 2
    cols = wq.shape[1]
    heads = cols // HEAD_DIM
    block = 2 * length
    wide = REACH * FAR
    span = block + 2 * wide
    rows = block // FAR
    near_rows = rows + 2 * FAR
    per = FAR // NEAR
    grans = block // GRAN
    tail = wide - block
    hbm = pl.BlockSpec(memory_space=pl.ANY)
    vmem = pl.BlockSpec(memory_space=pltpu.VMEM)
    v = pltpu.VMEM
    shapes = [((seqs, length, wo.shape[1]), BF16), ((seqs, heads, length), F32)]
    made = pl.pallas_call(
        functools.partial(layer_kernel, nsp),
        in_specs=[hbm] * 10,
        out_specs=[vmem, vmem],
        out_shape=[v(*shape) for shape in shapes],
        scratch_shapes=[
            v(tokens.shape, BF16), v(wq.shape, BF16), v(wk.shape, BF16), v(wv.shape, BF16),
            v(wo.shape, BF16), v((length, HEAD_DIM), F32), v((length, HEAD_DIM), F32),
            v((nsp, HEAD_DIM), F32), v((nsp, HEAD_DIM), F32), v(gain.shape, F32),
            v((half * heads, span, 2 * HEAD_DIM), BF16),
            v((half * heads, block, HEAD_DIM), BF16),
            v((half * heads, length, 2 * HEAD_DIM), BF16),
            v((half * heads, length, HEAD_DIM), BF16),
            v((ntp, seqs, heads, length, HEAD_DIM), BF16),
            v((half * heads, length, HEAD_DIM), BF16),
            v((seqs, heads, 1, length), F32),
            v((half * heads, 1, length), F32),
            v((2, 1, block), F32),
            v((2, FAR, (span - 2 * tail) // FAR, 2 * HEAD_DIM), BF16),
            v((2, FAR, rows, HEAD_DIM), BF16),
            v((2, block, HEAD_DIM), BF16),
            v((GRAN, GRAN), BF16), v((GRAN, GRAN), BF16),
            v((grans, GRAN, GRAN + 2 * REACH), F32),
            v((per * rows, per * near_rows), F32),
            v((rows, (span - 2 * tail) // FAR), F32),
            v((2 * (tail // GRAN), GRAN, tail), F32),
            v((2, FAR, rows, HEAD_DIM), F32),
            v((2, FAR, rows, HEAD_DIM), F32),
            v((2, FAR, rows, HEAD_DIM), F32),
            pltpu.SemaphoreType.DMA((seqs + 12,)),
            pltpu.SemaphoreType.DMA((24 * half * heads,)),
            pltpu.SemaphoreType.DMA((24 * half * heads,)),
        ],
        compiler_params=pltpu.CompilerParams(
            collective_id=0, has_side_effects=True, vmem_limit_bytes=52 * 2**20
        ),
        name="layer",
    )(*(
        pltpu.with_memory_space_constraint(a, pltpu.HBM)
        for a in (tokens, wq, wk, wv, wo, *tables, gain)
    ))
    return pl.pallas_call(
        emit_kernel,
        in_specs=[vmem, vmem],
        out_specs=[hbm, hbm],
        out_shape=[jax.ShapeDtypeStruct(*shape) for shape in shapes],
        scratch_shapes=[pltpu.SemaphoreType.DMA((len(shapes),))],
        name="emit",
    )(*(pltpu.with_memory_space_constraint(a, v) for a in made))


def emit_kernel(mixed, logs, mixed_h, logs_h, sems):
    pairs = ((mixed, mixed_h), (logs, logs_h))
    copies = [pltpu.make_async_copy(*pair, sems.at[n]) for n, pair in enumerate(pairs)]
    for c in copies:
        c.start()
    for c in copies:
        c.wait()


def shards(tokens, query_weight, key_weight, value_weight, out_gain, out_weight):
    length = tokens.shape[1]
    nsp = lax.axis_size("sp")
    frequency = ROPE_BASE ** (-np.arange(HEAD_DIM // 2) / (HEAD_DIM // 2))
    frequency = np.tile(frequency, 2)[None, :]
    step = np.arange(length)[:, None] * frequency
    base = (np.arange(nsp) * length)[:, None] * frequency
    tables = [
        jnp.asarray(f(a).astype(np.float32)) for a in (step, base) for f in (np.cos, np.sin)
    ]
    return tuple(
        layer(
            nsp, lax.axis_size("tp"), tokens, query_weight, key_weight, value_weight,
            out_weight, tables, out_gain[None, :],
        )
    )


def solution(mesh):
    return jax.shard_map(
        shards,
        mesh=mesh,
        in_specs=(
            P(None, "sp", None),
            P(None, "tp"),
            P(None, "tp"),
            P(None, "tp"),
            P(),
            P(None, "tp"),
        ),
        out_specs=(P(None, "sp", "tp"), P(None, "tp", "sp")),
        check_vma=False,
    )
```

```python
import functools
import math

import jax
import jax.numpy as jnp
import numpy as np
from jax import lax
from jax.experimental import pallas as pl
from jax.experimental.pallas import tpu as pltpu
from jax.sharding import PartitionSpec as P

HEAD_DIM = 128
REACH = 64
FAR = 16
NEAR = 4
GRAN = FAR * FAR
ROPE_BASE = 10000.0
MASK_FILL = -1e30
NORM_FLOOR = 1e-06
LOG2E = 1.0 / math.log(2.0)
LN2 = math.log(2.0)
F32 = jnp.float32
BF16 = jnp.bfloat16

MESH = pl.DeviceIdType.MESH


def iota(shape, dim):
    return lax.broadcasted_iota(jnp.int32, shape, dim)


def perm_token(p):
    slot = p // FAR
    a = p % FAR
    residue = slot // NEAR + NEAR * (slot % (FAR // NEAR))
    return a * FAR + residue


def dot_t(a, b):
    return lax.dot_general(a, b, (((1,), (1,)), ((), ())), preferred_element_type=F32)


def layer_kernel(
    nsp, tok_h, wq_h, wk_h, wv_h, wo_h, cos_h, sin_h, cos_base_h, sin_base_h, gain_h,
    out, log_out,
    tok, wq, wk, wv, wo, cos, sin, cos_base, sin_base, gain, kn, qn, kvs, qs, gath, outs, logs,
    lsend, lrow, kp, qp, on, perm, unperm, bias1, bias4, bias16, bias_end, o1, m1, l1,
    load_sem, send_sem, recv_sem,
):
    half = tok.shape[0] // 2
    units = kn.shape[0]
    length = tok.shape[1]
    block = 2 * length
    grans = block // GRAN
    wide = REACH * FAR
    side = wide // GRAN
    tail = wide - block
    span = block + 2 * wide
    rows = block // FAR
    ends = tail // GRAN
    key_rows = (span - 2 * tail) // FAR
    near_rows = rows + 2 * FAR
    cols = wq.shape[1]
    heads = cols // HEAD_DIM
    total = nsp * length
    scale = HEAD_DIM**-0.5 * LOG2E
    sp, t = lax.axis_index("sp"), lax.axis_index("tp")
    y, blk = sp % 2, sp // 2
    twin = sp + 1 - 2 * y
    x_peer = (t + 2) % 4
    d_peer = t + 1 - 2 * (t % 2)
    x_d_peer = (d_peer + 2) % 4
    mine, other = y * half, (1 - y) * half

    loads = []

    def load(src, dst):
        copy = pltpu.make_async_copy(src, dst, load_sem.at[len(loads)])
        copy.start()
        loads.append(copy)
        return copy

    cuts = (pl.ds(0, length // 3), pl.ds(length // 3, length - length // 3))
    got_first = [load(tok_h.at[mine, cuts[0]], tok.at[0, cuts[0]])]
    got_wk = load(wk_h, wk)
    got_tables = [
        load(*pair)
        for pair in (
            (cos_base_h, cos_base), (sin_base_h, sin_base), (cos_h, cos), (sin_h, sin)
        )
    ]
    got_wv = load(wv_h, wv)
    got_tok = {}

    barrier = pltpu.get_barrier_semaphore()
    has = {d: (sp + d >= 0) & (sp + d < nsp) for d in (2, -2, 4, -4)}
    reach = {d: has[d] & has[-d] for d in (2, -2)}
    beside = ((twin, t), (sp, x_peer), (sp, d_peer), (twin, x_peer))
    for peer in beside:
        pl.semaphore_signal(barrier, inc=1, device_id=peer, device_id_type=MESH)
    count = len(beside)
    for d in (2, -2):
        there = has[d]
        count = count + there.astype(jnp.int32)

        @pl.when(there)
        def _(d=d):
            pl.semaphore_signal(barrier, inc=1, device_id=(sp + d, t), device_id_type=MESH)

    first = pl.multiple_of(y * length, HEAD_DIM)
    second = pl.multiple_of((1 - y) * length, HEAD_DIM)

    def clear(d, at, size):
        @pl.when(jnp.logical_not(has[d]))
        def _():
            for u in range(units):
                kn[u, at : at + size] = jnp.zeros((size, kn.shape[2]), BF16)

    numbers, lane, sent = {}, [0], []

    def copy(name, src, dst, peer):
        n = numbers.setdefault(name, len(numbers))
        return pltpu.make_async_remote_copy(
            src_ref=src, dst_ref=dst, send_sem=send_sem.at[lane[0]], recv_sem=recv_sem.at[n],
            device_id=peer, device_id_type=MESH,
        )

    def when(there, act):
        act() if there is None else pl.when(there)(act)

    def drain():
        c, there, held = sent.pop(0)
        when(there, c.wait_send)
        return held

    def start(make, there=None):
        lane[0] = len(sent) if len(sent) < send_sem.shape[0] else drain()
        c = make()
        when(there, c.start)
        sent.append((c, there, lane[0]))

    def z_copy(kind, u, d, cut=None):
        if kind == "T":
            src = wide - tail if d > 0 else wide + block
            dst = 0 if d > 0 else span - tail
            size = tail
        else:
            if kind == "S":
                at, size = block - tail if d > 0 else 0, tail
            elif kind == "R":
                at, size = 0 if d > 0 else tail, block - tail
            else:
                at, size = first if kind == "A" else second, length
            if cut is not None:
                at, size = at + cut.start, cut.size
            src = wide + at
            dst = (tail if d > 0 else wide + block) + at
        pick = pl.ds(0, heads) if kind == "A" and u == 0 else u
        return copy(
            (kind, u, d, cut and cut.start), kn.at[pick, pl.ds(src, size)],
            kn.at[pick, pl.ds(dst, size)], (sp + d, t),
        )

    def z_start(kind, u, cut=None):
        for d in (2, -2):
            start(lambda: z_copy(kind, u, d, cut), reach[d] if kind == "T" else has[d])

    def z_wait(kind, u):
        for d in (2, -2):

            @pl.when(has[-2 * d] if kind == "T" else has[-d])
            def _():
                for cut in cuts if kind == "A" and u == 0 else (None,):
                    z_copy(kind, u, d, cut).wait_recv()

    every = pl.ds(0, length)

    def turned(x, w, store, cut=every):
        a = jnp.dot(x, w[...], preferred_element_type=F32)
        for h in range(heads):
            one = a[:, h * HEAD_DIM : (h + 1) * HEAD_DIM]
            other_half = pltpu.roll(one, HEAD_DIM // 2, 1)
            store(h, (one * cos[cut] + other_half * sin[cut]).astype(BF16))

    def lanes(n):
        return slice(n * HEAD_DIM, (n + 1) * HEAD_DIM)

    def keys_values(x, put, cut=every, ready=None):
        turned(x, wk, lambda h, a: put(2 * h, a), cut)
        if ready is not None:
            ready.wait()
        v = jnp.dot(x, wv[...], preferred_element_type=F32).astype(BF16)
        for h in range(heads):
            put(2 * h + 1, v[:, lanes(h)])

    def own_kv(s, cut=every, ready=None):
        def put(n, a):
            at = pl.ds(wide + first + cut.start, cut.size)
            kn[s * heads + n // 2, at, lanes(n % 2)] = a

        keys_values(tok[2 * s, cut], put, cut, ready)

    def twin_kv(s):
        def put(n, a):
            kvs[s * heads + n // 2, :, lanes(n % 2)] = a

        keys_values(tok[2 * s + 1], put)

    def own_q(s):
        def put(n, a):
            qn[s * heads + n, pl.ds(first, length)] = a

        turned(tok[2 * s], wq, put)

    def twin_q(s):
        def put(n, a):
            qs[s * heads + n] = a

        turned(tok[2 * s + 1], wq, put)

    def y_kv(u, at):
        return copy(("yk", u), kvs.at[u], kn.at[u, pl.ds(wide + at, length)], (twin, t))

    def y_q(s, at):
        pick = pl.ds(s * heads, heads)
        return copy(("yq", s), qs.at[pick], qn.at[pick, pl.ds(at, length)], (twin, t))

    def of(s):
        return range(s * heads, (s + 1) * heads)

    for c in got_tables:
        c.wait()
    cos_at, sin_at = cos_base[pl.ds(sp, 1)], sin_base[pl.ds(sp, 1)]
    sign = jnp.where(iota(cos.shape, 1) < HEAD_DIM // 2, -1.0, 1.0)
    cos_step, sin_step = cos[...], sin[...]
    cos[...] = cos_step * cos_at - sin_step * sin_at
    sin[...] = (sin_step * cos_at + cos_step * sin_at) * sign
    for c in (got_wk, got_first[0]):
        c.wait()
    got_first.append(load(tok_h.at[mine, cuts[1]], tok.at[0, cuts[1]]))
    got_tok["o", 0] = load(tok_h.at[other], tok.at[1])
    own_kv(0, cuts[0], got_wv)
    pl.semaphore_wait(barrier, count)
    z_start("A", 0, cuts[0])
    got_wq = load(wq_h, wq)
    got_first[1].wait()
    own_kv(0, cuts[1])
    z_start("A", 0, cuts[1])
    got_tok["o", 0].wait()
    for s in range(1, half):
        got_tok["o", s] = load(tok_h.at[other + s], tok.at[2 * s + 1])
        got_tok["m", s] = load(tok_h.at[mine + s], tok.at[2 * s])
    got_gain = load(gain_h, gain)
    got_wo = load(wo_h, wo)
    twin_kv(0)
    for u in of(0):
        start(lambda: y_kv(u, first))
    got_wq.wait()
    twin_q(0)
    start(lambda: y_q(0, first))
    for s in range(1, half):
        got_tok["o", s].wait()
        got_tok["m", s].wait()
        twin_kv(s)
        for u in of(s):
            start(lambda: y_kv(u, first))
        own_kv(s)
        twin_q(s)
        start(lambda: y_q(s, first))
    y_kv(0, second).wait_recv()
    z_start("B", 0)
    own_q(0)

    clear(-4, 0, tail)
    clear(-2, tail, block)
    clear(2, wide + block, block)
    clear(4, span - tail, tail)
    perm[...] = jnp.where(
        iota((GRAN, GRAN), 1) == perm_token(iota((GRAN, GRAN), 0)), 1.0, 0.0
    ).astype(BF16)
    unperm[...] = jnp.where(
        iota((GRAN, GRAN), 0) == perm_token(iota((GRAN, GRAN), 1)), 1.0, 0.0
    ).astype(BF16)
    kp[:, :, :, 2 * HEAD_DIM :] = jnp.ones((*kp.shape[:3], HEAD_DIM), BF16)
    origin = blk * block - wide
    shape = (GRAN, GRAN + 2 * REACH)
    token = perm_token(iota(shape, 0))
    for g in range(grans):
        q_at = wide + g * GRAN + token
        k_at = wide + g * GRAN - REACH + iota(shape, 1)
        ok = (jnp.abs(k_at - q_at) <= REACH) & (k_at + origin >= 0) & (k_at + origin < total)
        bias1[g] = jnp.where(ok, 0.0, MASK_FILL)
    per = FAR // NEAR
    shape = (per * rows, per * near_rows)
    row, col = iota(shape, 0), iota(shape, 1)
    q_at = (row % rows + side * FAR) * FAR + NEAR * (row // rows)
    k_at = (col % near_rows + (side - 1) * FAR) * FAR + NEAR * (col // near_rows)
    ok = (jnp.abs(k_at - q_at) <= REACH * NEAR) & (k_at + origin >= 0) & (k_at + origin < total)
    bias4[...] = jnp.where(ok, 0.0, MASK_FILL)
    shape = (rows, key_rows)
    q_at = iota(shape, 0) + side * FAR
    k_at = iota(shape, 1) + ends * FAR
    ok = (
        (jnp.abs(k_at - q_at) <= REACH)
        & (k_at * FAR + origin >= 0)
        & (k_at * FAR + origin < total)
    )
    bias16[...] = jnp.where(ok, 0.0, MASK_FILL)
    reached = [(0, 0), (grans - 1, span - tail)]
    shape = (GRAN, tail)
    token = perm_token(iota(shape, 0))
    for n, (g, at) in enumerate(reached):
        gap = at + iota(shape, 1) - (wide + g * GRAN + token)
        k_at = at + iota(shape, 1) + origin
        ok = (gap % FAR == 0) & (jnp.abs(gap) <= wide) & (k_at >= 0) & (k_at < total)
        bias_end[n] = jnp.where(ok, 0.0, MASK_FILL)

    y_kv(1, second).wait_recv()
    z_start("B", 1)
    for s in range(1, half):
        own_q(s)

    near_from, near_to = side - 1, side + grans + 1

    def gather_keys(u, slot, chunks):
        for j in chunks:
            moved = jnp.dot(
                perm[...], kn[u, j * GRAN : (j + 1) * GRAN], preferred_element_type=F32
            )
            moved = moved.astype(BF16).reshape(FAR, FAR, 2 * HEAD_DIM)
            at = (j - ends) * FAR
            kp[slot, :, at : at + FAR, : 2 * HEAD_DIM] = moved

    flat = (per * rows, HEAD_DIM)
    cube = (per, rows, HEAD_DIM)

    def merge(slot, sel, scores, weigh):
        m_old = m1[slot, sel].reshape(flat)
        m_new = jnp.maximum(m_old, jnp.max(scores, axis=1, keepdims=True))
        keep = jnp.exp2(m_old - m_new)
        p = jnp.exp2(scores - m_new[:, :1])
        o_l = weigh(p.astype(BF16))
        l = l1[slot, sel].reshape(flat) * keep + o_l[:, HEAD_DIM:]
        o = o1[slot, sel].reshape(flat) * keep + o_l[:, :HEAD_DIM]
        for ref, a in ((o1, o), (m1, m_new), (l1, l)):
            ref[slot, sel] = a.reshape(cube)

    def with_ones(v):
        return jnp.concatenate([v, jnp.ones_like(v)], axis=1)

    def attend_near(u):
        slot = u % 2
        if u % heads == 0:
            y_q(u // heads, second).wait_recv()
        gather_keys(u, slot, range(near_from, near_to))
        for g in range(grans):
            moved = jnp.dot(
                perm[...], qn[u, g * GRAN : (g + 1) * GRAN], preferred_element_type=F32
            )
            moved = moved.astype(BF16)
            qp[slot, :, g * FAR : (g + 1) * FAR] = moved.reshape(FAR, FAR, HEAD_DIM)
            at = wide + g * GRAN - REACH
            k = kn[u, at : at + GRAN + 2 * REACH, :HEAD_DIM]
            v = with_ones(kn[u, at : at + GRAN + 2 * REACH, HEAD_DIM:])
            sc = dot_t(moved, k) * scale + bias1[g]
            m = jnp.max(sc, axis=1, keepdims=True)
            p = jnp.exp2(sc - m)
            o_l = jnp.dot(p.astype(BF16), v, preferred_element_type=F32)
            o, l = o_l[:, :HEAD_DIM], o_l[:, HEAD_DIM:]
            for ref, a in ((o1, o), (m1, jnp.broadcast_to(m, o.shape)), (l1, l)):
                ref[slot, :, g * FAR : (g + 1) * FAR] = a.reshape(FAR, FAR, HEAD_DIM)

        near_at = (near_from - ends) * FAR
        for group in range(NEAR):
            sel = slice(group * per, (group + 1) * per)
            k4 = kp[slot, sel, near_at : near_at + near_rows, :HEAD_DIM].reshape(-1, HEAD_DIM)
            v4 = kp[slot, sel, near_at : near_at + near_rows, HEAD_DIM:].reshape(-1, 2 * HEAD_DIM)
            s4 = dot_t(qp[slot, sel].reshape(flat), k4) * scale + bias4[...]
            merge(slot, sel, s4, lambda p: jnp.dot(p, v4, preferred_element_type=F32))

    def attend_far(u):
        slot = u % 2
        gather_keys(u, slot, [*range(ends, near_from), *range(near_to, span // GRAN - ends)])
        for group in range(NEAR):
            sel = slice(group * per, (group + 1) * per)
            own = range(group * per, (group + 1) * per)
            b16 = bias16[...]
            s16 = [dot_t(qp[slot, r], kp[slot, r, :, :HEAD_DIM]) * scale + b16 for r in own]

            def weigh(p):
                return jnp.concatenate(
                    [
                        jnp.dot(
                            p[i * rows : (i + 1) * rows], kp[slot, r, :, HEAD_DIM:],
                            preferred_element_type=F32,
                        )
                        for i, r in enumerate(own)
                    ],
                    axis=0,
                )

            merge(slot, sel, jnp.concatenate(s16, axis=0), weigh)
        for g in range(ends, grans - ends):
            o, _, l = state(slot, g)
            settle(slot, g, o, l)

    def slots_of(g):
        return pl.ds(g * FAR, FAR)

    def state(slot, g):
        cut = slots_of(g)
        return [ref[slot, :, cut].reshape(GRAN, HEAD_DIM) for ref in (o1, m1, l1)]

    def settle(slot, g, o, l):
        merged = jnp.dot(unperm[...], (o / l).astype(BF16), preferred_element_type=F32)
        on[slot, pl.ds(g * GRAN, GRAN)] = merged.astype(BF16)

    def settle_log(slot, g):
        _, m, l = state(slot, g)
        x = m * LN2 + jnp.log(l)
        high = x.astype(BF16).astype(F32)
        mid = (x - high).astype(BF16).astype(F32)
        low = x - high - mid
        lane_at = iota((GRAN, HEAD_DIM), 1)
        terms = jnp.where(
            lane_at == 0, high, jnp.where(lane_at == 1, mid, jnp.where(lane_at == 2, low, 0.0))
        )
        pick = jnp.where(iota((FAR, HEAD_DIM), 0) == iota((FAR, HEAD_DIM), 1), 1.0, 0.0)
        turned_terms = dot_t(pick.astype(BF16), terms.astype(BF16)).astype(BF16)
        placed = jnp.dot(turned_terms, perm[...], preferred_element_type=F32)
        lrow[slot, :, g * GRAN : (g + 1) * GRAN] = jnp.sum(placed, axis=0, keepdims=True)

    def attend_side(u, n):
        slot = u % 2
        g, at = n * (grans - 1), n * (span - tail)
        if not isinstance(n, int):
            at = pl.multiple_of(at, GRAN)
        cut = slots_of(g)
        o_old, m_old, l_old = state(slot, g)
        q = qp[slot, :, cut].reshape(GRAN, HEAD_DIM)
        k = kn[u, pl.ds(at, tail), :HEAD_DIM]
        v = with_ones(kn[u, pl.ds(at, tail), HEAD_DIM:])
        sc = dot_t(q, k) * scale + bias_end[n]
        m = jnp.maximum(m_old, jnp.max(sc, axis=1, keepdims=True))
        keep = jnp.exp2(m_old - m)
        p = jnp.exp2(sc - m[:, :1])
        o_l = jnp.dot(p.astype(BF16), v, preferred_element_type=F32)
        l = l_old * keep + o_l[:, HEAD_DIM:]
        settle(slot, g, o_old * keep + o_l[:, :HEAD_DIM], l)
        m1[slot, :, cut] = m.reshape(FAR, FAR, HEAD_DIM)
        l1[slot, :, cut] = l.reshape(FAR, FAR, HEAD_DIM)

    def attend_end(u):
        z_wait("T", u)
        for n in range(len(reached)):
            attend_side(u, n)

    def some(part, half_at):
        if part is None:
            return every
        at = (1 - half_at) * tail if part == "mid" else half_at * (length - tail)
        size = length - tail if part == "mid" else tail
        return pl.ds(pl.multiple_of(at, HEAD_DIM), size)

    def across(u, base, half_at, part):
        cut = some(part, half_at)
        return copy(
            ("yo", u, part), outs.at[u, cut], gath.at[t, base + u // heads, u % heads, cut],
            (twin, t),
        )

    def log_across(s, base):
        return copy(("yl", s), lsend.at[pl.ds(s * heads, heads)], logs.at[base + s], (twin, t))

    def corner(u, part):
        cut = some(part, 1 - y)
        return copy(
            ("xr", u, part), outs.at[u, cut],
            gath.at[t, mine + u // heads, u % heads, cut], (twin, x_peer),
        )

    def piece(name, u, owner, base, peer, part):
        ref = gath.at[owner, base + u // heads, u % heads, some(part, y)]
        return copy((name, u, part), ref, ref, peer)

    def put(u, ref, half_at, part):
        cut = some(part, half_at)
        at = pl.multiple_of(half_at * length + cut.start, HEAD_DIM)
        ref[cut] = on[u % 2, pl.ds(at, cut.size)]

    def publish_twin(u, part=None):
        put(u, outs.at[u], 1 - y, part)
        start(lambda: corner(u, part))
        start(lambda: across(u, mine, 1 - y, part))

    def publish_own(u, part=None):
        s, h = u // heads, u % heads
        put(u, gath.at[t, mine + s, h], y, part)
        start(lambda: piece("xm", u, t, mine, (sp, x_peer), part))
        start(lambda: piece("dm", u, t, mine, (sp, d_peer), part))

    def publish_log(u):
        slot = u % 2
        s, h = u // heads, u % heads
        for g in range(grans):
            settle_log(slot, g)
        logs[mine + s, h] = lrow[slot, :, pl.ds(first, length)]
        lsend[u] = lrow[slot, :, pl.ds(second, length)]
        if h == heads - 1:
            start(lambda: log_across(s, mine))

    def publish(u):
        publish_twin(u)
        publish_own(u)
        publish_log(u)

    def spread(u, part=None):
        across(u, other, y, part).wait_recv()
        start(lambda: piece("dr", u, t, other, (sp, d_peer), part))
        piece("xm", u, x_peer, mine, (sp, x_peer), part).wait_recv()
        start(lambda: piece("em", u, x_peer, mine, (sp, d_peer), part))

    def spread_twin(u, part=None):
        piece("xr", u, x_peer, other, (sp, x_peer), part).wait_recv()
        start(lambda: piece("er", u, x_peer, other, (sp, d_peer), part))
        if part != "mid" and u % heads == heads - 1:
            log_across(u // heads, other).wait_recv()

    def finish(j, cut):
        acc = None
        square = None
        for n in range(gath.shape[0]):
            x = jnp.concatenate([gath[n, j, h, cut] for h in range(heads)], axis=1).astype(F32)
            at = slice(n * cols, (n + 1) * cols)
            scaled = (x * gain[:, at]).astype(BF16)
            term = jnp.dot(scaled, wo[at], preferred_element_type=F32)
            sq = jnp.sum(x * x, axis=1, keepdims=True)
            acc = term if acc is None else acc + term
            square = sq if square is None else square + sq
        out[j, cut] = (acc * lax.rsqrt(square / wo.shape[0] + NORM_FLOOR)).astype(BF16)

    def finish_mine(s, part=None):
        for u in of(s):
            for p in parts_of(u, part):
                piece("dm", u, d_peer, mine, (sp, d_peer), p).wait_recv()
                piece("em", u, x_d_peer, mine, (sp, d_peer), p).wait_recv()
        finish(mine + s, some(part, y))

    def finish_other(s, part=None):
        for u in of(s):
            for p in parts_of(u, part):
                piece("dr", u, d_peer, other, (sp, d_peer), p).wait_recv()
                piece("er", u, x_d_peer, other, (sp, d_peer), p).wait_recv()
        finish(other + s, some(part, y))

    def parts_of(u, part):
        if u == units - 1:
            return (part,)
        return () if part == "end" else (None,)

    def arrived(u):
        if u == 0 or u >= heads:
            z_wait("A", u)
        z_wait("B", u)

    arrived(0)
    z_start("T", 0)
    z_start("A", 2)
    attend_near(0)
    attend_far(0)
    arrived(1)
    z_start("T", 1)
    attend_near(1)
    y_kv(2, second).wait_recv()
    z_start("B", 2)
    attend_end(0)
    publish(0)
    attend_far(1)
    y_kv(3, second).wait_recv()
    z_start("S", 3)
    attend_end(1)
    publish(1)
    arrived(2)
    z_start("T", 2)
    z_start("R", 3)
    attend_near(2)
    attend_far(2)
    z_wait("S", 3)
    z_start("T", 3)
    spread(0)
    spread_twin(0)
    got_gain.wait()
    got_wo.wait()
    attend_end(2)
    publish(2)
    attend_near(3)
    spread(1)
    spread_twin(1)
    z_wait("R", 3)
    attend_far(3)
    publish_twin(3, "mid")
    publish_own(3, "mid")
    finish_mine(0)
    z_wait("T", 3)
    attend_side(3, 1 - y)
    publish_twin(3, "end")
    attend_side(3, y)
    publish_own(3, "end")
    publish_log(3)
    finish_other(0)
    spread(2)
    spread_twin(2)
    spread(3, "mid")
    spread_twin(3, "mid")
    finish_mine(1, "mid")
    finish_other(1, "mid")
    spread(3, "end")
    spread_twin(3, "end")
    finish_mine(1, "end")
    finish_other(1, "end")
    for j in range(logs.shape[0]):
        for h in range(heads):
            log_out[j, h : h + 1] = logs[j, h]
    while sent:
        drain()


def layer(nsp, ntp, tokens, wq, wk, wv, wo, tables, gain):
    seqs, length, width = tokens.shape
    half = seqs // 2
    cols = wq.shape[1]
    heads = cols // HEAD_DIM
    block = 2 * length
    wide = REACH * FAR
    span = block + 2 * wide
    rows = block // FAR
    near_rows = rows + 2 * FAR
    per = FAR // NEAR
    grans = block // GRAN
    tail = wide - block
    hbm = pl.BlockSpec(memory_space=pl.ANY)
    vmem = pl.BlockSpec(memory_space=pltpu.VMEM)
    v = pltpu.VMEM
    shapes = [((seqs, length, wo.shape[1]), BF16), ((seqs, heads, length), F32)]
    made = pl.pallas_call(
        functools.partial(layer_kernel, nsp),
        in_specs=[hbm] * 10,
        out_specs=[vmem, vmem],
        out_shape=[v(*shape) for shape in shapes],
        scratch_shapes=[
            v(tokens.shape, BF16), v(wq.shape, BF16), v(wk.shape, BF16), v(wv.shape, BF16),
            v(wo.shape, BF16), v((length, HEAD_DIM), F32), v((length, HEAD_DIM), F32),
            v((nsp, HEAD_DIM), F32), v((nsp, HEAD_DIM), F32), v(gain.shape, F32),
            v((half * heads, span, 2 * HEAD_DIM), BF16),
            v((half * heads, block, HEAD_DIM), BF16),
            v((half * heads, length, 2 * HEAD_DIM), BF16),
            v((half * heads, length, HEAD_DIM), BF16),
            v((ntp, seqs, heads, length, HEAD_DIM), BF16),
            v((half * heads, length, HEAD_DIM), BF16),
            v((seqs, heads, 1, length), F32),
            v((half * heads, 1, length), F32),
            v((2, 1, block), F32),
            v((2, FAR, (span - 2 * tail) // FAR, 3 * HEAD_DIM), BF16),
            v((2, FAR, rows, HEAD_DIM), BF16),
            v((2, block, HEAD_DIM), BF16),
            v((GRAN, GRAN), BF16), v((GRAN, GRAN), BF16),
            v((grans, GRAN, GRAN + 2 * REACH), F32),
            v((per * rows, per * near_rows), F32),
            v((rows, (span - 2 * tail) // FAR), F32),
            v((2 * (tail // GRAN), GRAN, tail), F32),
            v((2, FAR, rows, HEAD_DIM), F32),
            v((2, FAR, rows, HEAD_DIM), F32),
            v((2, FAR, rows, HEAD_DIM), F32),
            pltpu.SemaphoreType.DMA((seqs + 10,)),
            pltpu.SemaphoreType.DMA((6 * half * heads,)),
            pltpu.SemaphoreType.DMA((16 * half * heads + 3,)),
        ],
        compiler_params=pltpu.CompilerParams(
            collective_id=0, has_side_effects=True, vmem_limit_bytes=52 * 2**20
        ),
        name="layer",
    )(*(
        pltpu.with_memory_space_constraint(a, pltpu.HBM)
        for a in (tokens, wq, wk, wv, wo, *tables, gain)
    ))
    return pl.pallas_call(
        emit_kernel,
        in_specs=[vmem, vmem],
        out_specs=[hbm, hbm],
        out_shape=[jax.ShapeDtypeStruct(*shape) for shape in shapes],
        scratch_shapes=[pltpu.SemaphoreType.DMA((len(shapes),))],
        name="emit",
    )(*(pltpu.with_memory_space_constraint(a, v) for a in made))


def emit_kernel(mixed, logs, mixed_h, logs_h, sems):
    pairs = ((mixed, mixed_h), (logs, logs_h))
    copies = [pltpu.make_async_copy(*pair, sems.at[n]) for n, pair in enumerate(pairs)]
    for c in copies:
        c.start()
    for c in copies:
        c.wait()


def shards(tokens, query_weight, key_weight, value_weight, out_gain, out_weight):
    length = tokens.shape[1]
    nsp = lax.axis_size("sp")
    frequency = ROPE_BASE ** (-np.arange(HEAD_DIM // 2) / (HEAD_DIM // 2))
    frequency = np.tile(frequency, 2)[None, :]
    step = np.arange(length)[:, None] * frequency
    base = (np.arange(nsp) * length)[:, None] * frequency
    tables = [
        jnp.asarray(f(a).astype(np.float32)) for a in (step, base) for f in (np.cos, np.sin)
    ]
    return tuple(
        layer(
            nsp, lax.axis_size("tp"), tokens, query_weight, key_weight, value_weight,
            out_weight, tables, out_gain[None, :],
        )
    )


def solution(mesh):
    return jax.shard_map(
        shards,
        mesh=mesh,
        in_specs=(
            P(None, "sp", None),
            P(None, "tp"),
            P(None, "tp"),
            P(None, "tp"),
            P(),
            P(None, "tp"),
        ),
        out_specs=(P(None, "sp", "tp"), P(None, "tp", "sp")),
        check_vma=False,
    )
```

```python
import functools
import math

import jax
import jax.numpy as jnp
import numpy as np
from jax import lax
from jax.experimental import pallas as pl
from jax.experimental.pallas import tpu as pltpu
from jax.sharding import PartitionSpec as P

HEAD_DIM = 128
REACH = 64
FAR = 16
NEAR = 4
GRAN = FAR * FAR
ROPE_BASE = 10000.0
MASK_FILL = -1e30
NORM_FLOOR = 1e-06
LOG2E = 1.0 / math.log(2.0)
LN2 = math.log(2.0)
F32 = jnp.float32
BF16 = jnp.bfloat16

MESH = pl.DeviceIdType.MESH


def iota(shape, dim):
    return lax.broadcasted_iota(jnp.int32, shape, dim)


def perm_token(p):
    slot = p // FAR
    a = p % FAR
    residue = slot // NEAR + NEAR * (slot % (FAR // NEAR))
    return a * FAR + residue


def dot_t(a, b):
    return lax.dot_general(a, b, (((1,), (1,)), ((), ())), preferred_element_type=F32)


def layer_kernel(
    nsp, tok_h, wq_h, wk_h, wv_h, wo_h, cos_h, sin_h, cos_base_h, sin_base_h, gain_h,
    out, log_out,
    tok, wq, wkv, wo, cos, sin, cos_base, sin_base, gain, kn, qn, kvs, qs, gath, outs, logs,
    lsend, lrow, kp, qp, on, perm, unperm, bias1, bias4, bias16, bias_end, o1, m1, l1,
    load_sem, send_sem, recv_sem,
):
    half = tok.shape[0] // 2
    units = kn.shape[0]
    length = tok.shape[1]
    block = 2 * length
    grans = block // GRAN
    wide = REACH * FAR
    side = wide // GRAN
    tail = wide - block
    span = block + 2 * wide
    rows = block // FAR
    ends = tail // GRAN
    key_rows = (span - 2 * tail) // FAR
    near_rows = rows + 2 * FAR
    cols = wq.shape[1]
    heads = cols // HEAD_DIM
    total = nsp * length
    scale = HEAD_DIM**-0.5 * LOG2E
    sp, t = lax.axis_index("sp"), lax.axis_index("tp")
    y, blk = sp % 2, sp // 2
    twin = sp + 1 - 2 * y
    x_peer = (t + 2) % 4
    d_peer = t + 1 - 2 * (t % 2)
    x_d_peer = (d_peer + 2) % 4
    mine, other = y * half, (1 - y) * half

    def lanes(n):
        return slice(n * HEAD_DIM, (n + 1) * HEAD_DIM)

    loads = []

    def load(src, dst):
        copy = pltpu.make_async_copy(src, dst, load_sem.at[len(loads)])
        copy.start()
        loads.append(copy)
        return copy

    cuts = (pl.ds(0, length // 3), pl.ds(length // 3, length - length // 3))
    got_first = [load(tok_h.at[mine, cuts[0]], tok.at[0, cuts[0]])]

    def load_kv(h):
        cut = lanes(h)
        got = [load(wk_h.at[:, cut], wkv.at[:, lanes(2 * h)])]
        return [*got, load(wv_h.at[:, cut], wkv.at[:, lanes(2 * h + 1)])]

    got_kv = [load_kv(0)]
    got_tables = [
        load(*pair)
        for pair in (
            (cos_base_h, cos_base), (sin_base_h, sin_base), (cos_h, cos), (sin_h, sin)
        )
    ]
    got_kv += [load_kv(h) for h in range(1, heads)]
    got_tok = {}

    barrier = pltpu.get_barrier_semaphore()
    has = {d: (sp + d >= 0) & (sp + d < nsp) for d in (2, -2, 4, -4)}
    reach = {d: has[d] & has[-d] for d in (2, -2)}
    beside = ((twin, t), (sp, x_peer), (sp, d_peer), (twin, x_peer))
    for peer in beside:
        pl.semaphore_signal(barrier, inc=1, device_id=peer, device_id_type=MESH)
    count = len(beside)
    for d in (2, -2):
        there = has[d]
        count = count + there.astype(jnp.int32)

        @pl.when(there)
        def _(d=d):
            pl.semaphore_signal(barrier, inc=1, device_id=(sp + d, t), device_id_type=MESH)

    first = pl.multiple_of(y * length, HEAD_DIM)
    second = pl.multiple_of((1 - y) * length, HEAD_DIM)

    def clear(d, at, size):
        @pl.when(jnp.logical_not(has[d]))
        def _():
            for u in range(units):
                kn[u, at : at + size] = jnp.zeros((size, kn.shape[2]), BF16)

    numbers, lane, sent = {}, [0], []

    def copy(name, src, dst, peer):
        n = numbers.setdefault(name, len(numbers))
        return pltpu.make_async_remote_copy(
            src_ref=src, dst_ref=dst, send_sem=send_sem.at[lane[0]], recv_sem=recv_sem.at[n],
            device_id=peer, device_id_type=MESH,
        )

    def when(there, act):
        act() if there is None else pl.when(there)(act)

    def drain():
        c, there, held = sent.pop(0)
        when(there, c.wait_send)
        return held

    def start(make, there=None):
        lane[0] = len(sent) if len(sent) < send_sem.shape[0] else drain()
        c = make()
        when(there, c.start)
        sent.append((c, there, lane[0]))

    opening = [(h, cuts[0]) for h in range(heads)] + [(pl.ds(0, heads), cuts[1])]

    def z_copy(kind, u, d, n=None):
        pick = u
        if kind == "T":
            src = wide - tail if d > 0 else wide + block
            dst = 0 if d > 0 else span - tail
            size = tail
        else:
            if kind == "S":
                at, size = block - tail if d > 0 else 0, tail
            elif kind == "R":
                at, size = 0 if d > 0 else tail, block - tail
            else:
                at, size = first if kind == "A" else second, length
            if n is not None:
                pick, cut = opening[n]
                at, size = at + cut.start, cut.size
            src = wide + at
            dst = (tail if d > 0 else wide + block) + at
        return copy(
            (kind, u, d, n), kn.at[pick, pl.ds(src, size)], kn.at[pick, pl.ds(dst, size)], (sp + d, t)
        )

    def z_start(kind, u, n=None, also=True):
        for d in (2, -2):
            start(lambda: z_copy(kind, u, d, n), also & (reach[d] if kind == "T" else has[d]))

    def z_wait(kind, u):
        for d in (2, -2):

            @pl.when(has[-2 * d] if kind == "T" else has[-d])
            def _():
                for n in range(len(opening)) if kind == "A" and u == 0 else (None,):
                    z_copy(kind, u, d, n).wait_recv()

    every = pl.ds(0, length)

    def rotated(one, cut):
        other_half = pltpu.roll(one, HEAD_DIM // 2, 1)
        return (one * cos[cut] + other_half * sin[cut]).astype(BF16)

    def turned(x, w, store):
        a = jnp.dot(x, w[...], preferred_element_type=F32)
        for h in range(heads):
            store(h, rotated(a[:, lanes(h)], every))

    def keys_values(x, put, cut=every, of_heads=range(heads)):
        for h in of_heads:
            a = jnp.dot(
                x, wkv[:, 2 * h * HEAD_DIM : (2 * h + 2) * HEAD_DIM], preferred_element_type=F32
            )
            put(2 * h, rotated(a[:, :HEAD_DIM], cut))
            put(2 * h + 1, a[:, HEAD_DIM:].astype(BF16))

    def own_kv(s, cut=every, of_heads=range(heads)):
        def put(n, a):
            at = pl.ds(wide + first + cut.start, cut.size)
            kn[s * heads + n // 2, at, lanes(n % 2)] = a

        keys_values(tok[2 * s, cut], put, cut, of_heads)

    def twin_kv(s):
        def put(n, a):
            kvs[s * heads + n // 2, :, lanes(n % 2)] = a

        keys_values(tok[2 * s + 1], put)

    def own_q(s):
        def put(n, a):
            qn[s * heads + n, pl.ds(first, length)] = a

        turned(tok[2 * s], wq, put)

    def twin_q(s):
        def put(n, a):
            qs[s * heads + n] = a

        turned(tok[2 * s + 1], wq, put)

    def y_kv(u, at):
        return copy(("yk", u), kvs.at[u], kn.at[u, pl.ds(wide + at, length)], (twin, t))

    def y_q(s, at):
        pick = pl.ds(s * heads, heads)
        return copy(("yq", s), qs.at[pick], qn.at[pick, pl.ds(at, length)], (twin, t))

    def of(s):
        return range(s * heads, (s + 1) * heads)

    for c in got_tables:
        c.wait()
    cos_at, sin_at = cos_base[pl.ds(sp, 1)], sin_base[pl.ds(sp, 1)]

    def angles(cut):
        sign = jnp.where(iota((cut.size, HEAD_DIM), 1) < HEAD_DIM // 2, -1.0, 1.0)
        cos_step, sin_step = cos[cut], sin[cut]
        cos[cut] = cos_step * cos_at - sin_step * sin_at
        sin[cut] = (sin_step * cos_at + cos_step * sin_at) * sign

    angles(cuts[0])
    got_first[0].wait()
    for h in range(heads):
        for c in got_kv[h]:
            c.wait()
        if h == 0:
            got_first.append(load(tok_h.at[mine, cuts[1]], tok.at[0, cuts[1]]))
            got_tok["o", 0] = load(tok_h.at[other], tok.at[1])
        own_kv(0, cuts[0], [h])
        if h == 0:
            pl.semaphore_wait(barrier, count)
        z_start("A", 0, h)
    angles(cuts[1])
    got_wq = load(wq_h, wq)
    got_first[1].wait()
    own_kv(0, cuts[1])
    z_start("A", 0, heads)
    got_tok["o", 0].wait()
    for s in range(1, half):
        got_tok["o", s] = load(tok_h.at[other + s], tok.at[2 * s + 1])
        got_tok["m", s] = load(tok_h.at[mine + s], tok.at[2 * s])
    got_gain = load(gain_h, gain)
    got_wo = load(wo_h, wo)
    twin_kv(0)
    for u in of(0):
        start(lambda: y_kv(u, first))
    got_wq.wait()
    twin_q(0)
    start(lambda: y_q(0, first))
    for s in range(1, half):
        got_tok["o", s].wait()
        got_tok["m", s].wait()
        twin_kv(s)
        for u in of(s):
            start(lambda: y_kv(u, first))
        own_kv(s)
        twin_q(s)
        start(lambda: y_q(s, first))
    y_kv(0, second).wait_recv()
    z_start("B", 0)
    own_q(0)

    clear(-4, 0, tail)
    clear(-2, tail, block)
    clear(2, wide + block, block)
    clear(4, span - tail, tail)
    perm[...] = jnp.where(
        iota((GRAN, GRAN), 1) == perm_token(iota((GRAN, GRAN), 0)), 1.0, 0.0
    ).astype(BF16)
    unperm[...] = jnp.where(
        iota((GRAN, GRAN), 0) == perm_token(iota((GRAN, GRAN), 1)), 1.0, 0.0
    ).astype(BF16)
    kp[:, :, :, 2 * HEAD_DIM :] = jnp.ones((*kp.shape[:3], HEAD_DIM), BF16)
    origin = blk * block - wide
    shape = (GRAN, GRAN + 2 * REACH)
    token = perm_token(iota(shape, 0))
    for g in range(grans):
        q_at = wide + g * GRAN + token
        k_at = wide + g * GRAN - REACH + iota(shape, 1)
        ok = (jnp.abs(k_at - q_at) <= REACH) & (k_at + origin >= 0) & (k_at + origin < total)
        bias1[g] = jnp.where(ok, 0.0, MASK_FILL)
    per = FAR // NEAR
    shape = (per * rows, per * near_rows)
    row, col = iota(shape, 0), iota(shape, 1)
    q_at = (row % rows + side * FAR) * FAR + NEAR * (row // rows)
    k_at = (col % near_rows + (side - 1) * FAR) * FAR + NEAR * (col // near_rows)
    ok = (jnp.abs(k_at - q_at) <= REACH * NEAR) & (k_at + origin >= 0) & (k_at + origin < total)
    bias4[...] = jnp.where(ok, 0.0, MASK_FILL)
    shape = (rows, key_rows)
    q_at = iota(shape, 0) + side * FAR
    k_at = iota(shape, 1) + ends * FAR
    ok = (
        (jnp.abs(k_at - q_at) <= REACH)
        & (k_at * FAR + origin >= 0)
        & (k_at * FAR + origin < total)
    )
    bias16[...] = jnp.where(ok, 0.0, MASK_FILL)
    reached = [(0, 0), (grans - 1, span - tail)]
    shape = (GRAN, tail)
    token = perm_token(iota(shape, 0))
    for n, (g, at) in enumerate(reached):
        gap = at + iota(shape, 1) - (wide + g * GRAN + token)
        k_at = at + iota(shape, 1) + origin
        ok = (gap % FAR == 0) & (jnp.abs(gap) <= wide) & (k_at >= 0) & (k_at < total)
        bias_end[n] = jnp.where(ok, 0.0, MASK_FILL)

    y_kv(1, second).wait_recv()
    z_start("B", 1)
    for s in range(1, half):
        own_q(s)

    near_from, near_to = side - 1, side + grans + 1

    def gather_keys(u, slot, chunks):
        for j in chunks:
            moved = jnp.dot(
                perm[...], kn[u, j * GRAN : (j + 1) * GRAN], preferred_element_type=F32
            )
            moved = moved.astype(BF16).reshape(FAR, FAR, 2 * HEAD_DIM)
            at = (j - ends) * FAR
            kp[slot, :, at : at + FAR, : 2 * HEAD_DIM] = moved

    flat = (per * rows, HEAD_DIM)
    cube = (per, rows, HEAD_DIM)

    def merge(slot, sel, scores, weigh):
        m_old = m1[slot, sel].reshape(flat)
        m_new = jnp.maximum(m_old, jnp.max(scores, axis=1, keepdims=True))
        keep = jnp.exp2(m_old - m_new)
        p = jnp.exp2(scores - m_new[:, :1])
        o_l = weigh(p.astype(BF16))
        l = l1[slot, sel].reshape(flat) * keep + o_l[:, HEAD_DIM:]
        o = o1[slot, sel].reshape(flat) * keep + o_l[:, :HEAD_DIM]
        for ref, a in ((o1, o), (m1, m_new), (l1, l)):
            ref[slot, sel] = a.reshape(cube)

    def with_ones(v):
        return jnp.concatenate([v, jnp.ones_like(v)], axis=1)

    def attend_near(u):
        slot = u % 2
        if u % heads == 0:
            y_q(u // heads, second).wait_recv()
        gather_keys(u, slot, range(near_from, near_to))
        for g in range(grans):
            moved = jnp.dot(
                perm[...], qn[u, g * GRAN : (g + 1) * GRAN], preferred_element_type=F32
            )
            moved = moved.astype(BF16)
            qp[slot, :, g * FAR : (g + 1) * FAR] = moved.reshape(FAR, FAR, HEAD_DIM)
            at = wide + g * GRAN - REACH
            k = kn[u, at : at + GRAN + 2 * REACH, :HEAD_DIM]
            v = with_ones(kn[u, at : at + GRAN + 2 * REACH, HEAD_DIM:])
            sc = dot_t(moved, k) * scale + bias1[g]
            m = jnp.max(sc, axis=1, keepdims=True)
            p = jnp.exp2(sc - m)
            o_l = jnp.dot(p.astype(BF16), v, preferred_element_type=F32)
            o, l = o_l[:, :HEAD_DIM], o_l[:, HEAD_DIM:]
            for ref, a in ((o1, o), (m1, jnp.broadcast_to(m, o.shape)), (l1, l)):
                ref[slot, :, g * FAR : (g + 1) * FAR] = a.reshape(FAR, FAR, HEAD_DIM)

        near_at = (near_from - ends) * FAR
        for group in range(NEAR):
            sel = slice(group * per, (group + 1) * per)
            k4 = kp[slot, sel, near_at : near_at + near_rows, :HEAD_DIM].reshape(-1, HEAD_DIM)
            v4 = kp[slot, sel, near_at : near_at + near_rows, HEAD_DIM:].reshape(-1, 2 * HEAD_DIM)
            s4 = dot_t(qp[slot, sel].reshape(flat), k4) * scale + bias4[...]
            merge(slot, sel, s4, lambda p: jnp.dot(p, v4, preferred_element_type=F32))

    def attend_far(u):
        slot = u % 2
        gather_keys(u, slot, [*range(ends, near_from), *range(near_to, span // GRAN - ends)])
        for group in range(NEAR):
            sel = slice(group * per, (group + 1) * per)
            own = range(group * per, (group + 1) * per)
            b16 = bias16[...]
            s16 = [dot_t(qp[slot, r], kp[slot, r, :, :HEAD_DIM]) * scale + b16 for r in own]

            def weigh(p):
                return jnp.concatenate(
                    [
                        jnp.dot(
                            p[i * rows : (i + 1) * rows], kp[slot, r, :, HEAD_DIM:],
                            preferred_element_type=F32,
                        )
                        for i, r in enumerate(own)
                    ],
                    axis=0,
                )

            merge(slot, sel, jnp.concatenate(s16, axis=0), weigh)
        for g in range(ends, grans - ends):
            o, _, l = state(slot, g)
            settle(slot, g, o, l)

    def slots_of(g):
        return pl.ds(g * FAR, FAR)

    def state(slot, g):
        cut = slots_of(g)
        return [ref[slot, :, cut].reshape(GRAN, HEAD_DIM) for ref in (o1, m1, l1)]

    def settle(slot, g, o, l):
        merged = jnp.dot(unperm[...], (o / l).astype(BF16), preferred_element_type=F32)
        on[slot, pl.ds(g * GRAN, GRAN)] = merged.astype(BF16)

    def settle_log(slot, g):
        _, m, l = state(slot, g)
        x = m * LN2 + jnp.log(l)
        high = x.astype(BF16).astype(F32)
        mid = (x - high).astype(BF16).astype(F32)
        low = x - high - mid
        lane_at = iota((GRAN, HEAD_DIM), 1)
        terms = jnp.where(
            lane_at == 0, high, jnp.where(lane_at == 1, mid, jnp.where(lane_at == 2, low, 0.0))
        )
        pick = jnp.where(iota((FAR, HEAD_DIM), 0) == iota((FAR, HEAD_DIM), 1), 1.0, 0.0)
        turned_terms = dot_t(pick.astype(BF16), terms.astype(BF16)).astype(BF16)
        placed = jnp.dot(turned_terms, perm[...], preferred_element_type=F32)
        lrow[slot, :, g * GRAN : (g + 1) * GRAN] = jnp.sum(placed, axis=0, keepdims=True)

    def attend_side(u, n):
        slot = u % 2
        g, at = n * (grans - 1), n * (span - tail)
        if not isinstance(n, int):
            at = pl.multiple_of(at, GRAN)
        cut = slots_of(g)
        o_old, m_old, l_old = state(slot, g)
        q = qp[slot, :, cut].reshape(GRAN, HEAD_DIM)
        k = kn[u, pl.ds(at, tail), :HEAD_DIM]
        v = with_ones(kn[u, pl.ds(at, tail), HEAD_DIM:])
        sc = dot_t(q, k) * scale + bias_end[n]
        m = jnp.maximum(m_old, jnp.max(sc, axis=1, keepdims=True))
        keep = jnp.exp2(m_old - m)
        p = jnp.exp2(sc - m[:, :1])
        o_l = jnp.dot(p.astype(BF16), v, preferred_element_type=F32)
        l = l_old * keep + o_l[:, HEAD_DIM:]
        settle(slot, g, o_old * keep + o_l[:, :HEAD_DIM], l)
        m1[slot, :, cut] = m.reshape(FAR, FAR, HEAD_DIM)
        l1[slot, :, cut] = l.reshape(FAR, FAR, HEAD_DIM)

    def attend_end(u):
        z_wait("T", u)
        for n in range(len(reached)):
            attend_side(u, n)

    def some(part, half_at):
        if part is None:
            return every
        at = (1 - half_at) * tail if part == "mid" else half_at * (length - tail)
        size = length - tail if part == "mid" else tail
        return pl.ds(pl.multiple_of(at, HEAD_DIM), size)

    def across(u, base, half_at, part):
        cut = some(part, half_at)
        return copy(
            ("yo", u, part), outs.at[u, cut], gath.at[t, base + u // heads, u % heads, cut],
            (twin, t),
        )

    def log_across(s, base):
        return copy(("yl", s), lsend.at[pl.ds(s * heads, heads)], logs.at[base + s], (twin, t))

    def corner(u, part):
        cut = some(part, 1 - y)
        return copy(
            ("xr", u, part), outs.at[u, cut],
            gath.at[t, mine + u // heads, u % heads, cut], (twin, x_peer),
        )

    def piece(name, u, owner, base, peer, part):
        ref = gath.at[owner, base + u // heads, u % heads, some(part, y)]
        return copy((name, u, part), ref, ref, peer)

    def put(u, ref, half_at, part):
        cut = some(part, half_at)
        at = pl.multiple_of(half_at * length + cut.start, HEAD_DIM)
        ref[cut] = on[u % 2, pl.ds(at, cut.size)]

    def publish_twin(u, part=None):
        put(u, outs.at[u], 1 - y, part)
        start(lambda: corner(u, part))
        start(lambda: across(u, mine, 1 - y, part))

    def publish_own(u, part=None):
        s, h = u // heads, u % heads
        put(u, gath.at[t, mine + s, h], y, part)
        start(lambda: piece("xm", u, t, mine, (sp, x_peer), part))
        start(lambda: piece("dm", u, t, mine, (sp, d_peer), part))

    def publish_log(u):
        slot = u % 2
        s, h = u // heads, u % heads
        for g in range(grans):
            settle_log(slot, g)
        logs[mine + s, h] = lrow[slot, :, pl.ds(first, length)]
        lsend[u] = lrow[slot, :, pl.ds(second, length)]
        if h == heads - 1:
            start(lambda: log_across(s, mine))

    def publish(u):
        publish_twin(u)
        publish_own(u)
        publish_log(u)

    def spread(u, part=None):
        across(u, other, y, part).wait_recv()
        start(lambda: piece("dr", u, t, other, (sp, d_peer), part))
        piece("xm", u, x_peer, mine, (sp, x_peer), part).wait_recv()
        start(lambda: piece("em", u, x_peer, mine, (sp, d_peer), part))

    def spread_twin(u, part=None):
        piece("xr", u, x_peer, other, (sp, x_peer), part).wait_recv()
        start(lambda: piece("er", u, x_peer, other, (sp, d_peer), part))
        if part != "mid" and u % heads == heads - 1:
            log_across(u // heads, other).wait_recv()

    def finish(js, cut):
        acc = None
        squares = None
        for n in range(gath.shape[0]):
            xs = [
                jnp.concatenate([gath[n, j, h, cut] for j in js], axis=0).astype(F32)
                for h in range(heads)
            ]
            at = slice(n * cols, (n + 1) * cols)
            scaled = (jnp.concatenate(xs, axis=1) * gain[:, at]).astype(BF16)
            term = jnp.dot(scaled, wo[at], preferred_element_type=F32)
            acc = term if acc is None else acc + term
            for x in xs:
                squares = x * x if squares is None else squares + x * x
        square = jnp.sum(squares, axis=1, keepdims=True)
        a = (acc * lax.rsqrt(square / wo.shape[0] + NORM_FLOOR)).astype(BF16)
        for n, j in enumerate(js):
            out[j, cut] = a[n * cut.size : (n + 1) * cut.size]

    def finish_seq(s, part=None):
        for kinds, base in ((("dm", "em"), mine), (("dr", "er"), other)):
            for u in of(s):
                for p in parts_of(u, part):
                    for kind, owner in zip(kinds, (d_peer, x_d_peer)):
                        piece(kind, u, owner, base, (sp, d_peer), p).wait_recv()
        finish((mine + s, other + s), some(part, y))

    def parts_of(u, part):
        if u == units - 1:
            return (part,)
        return () if part == "end" else (None,)

    def arrived(u):
        if u == 0 or u >= heads:
            z_wait("A", u)
        z_wait("B", u)

    arrived(0)
    z_start("T", 0)
    z_start("A", 2)
    attend_near(0)
    attend_far(0)
    arrived(1)
    z_start("T", 1)
    attend_near(1)
    y_kv(2, second).wait_recv()
    z_start("B", 2)
    attend_end(0)
    publish(0)
    attend_far(1)
    y_kv(3, second).wait_recv()
    z_start("S", 3)
    attend_end(1)
    publish(1)
    arrived(2)
    z_start("T", 2)
    z_start("R", 3)
    attend_near(2)
    attend_far(2)
    z_wait("S", 3)
    z_start("T", 3, also=t % 2 == 0)
    attend_near(3)
    attend_end(2)
    publish(2)
    spread(0)
    spread_twin(0)
    spread(1)
    spread_twin(1)
    z_wait("R", 3)
    z_start("T", 3, also=t % 2 == 1)
    attend_far(3)
    publish_twin(3, "mid")
    publish_own(3, "mid")
    z_wait("T", 3)
    attend_side(3, 1 - y)
    publish_twin(3, "end")
    attend_side(3, y)
    publish_own(3, "end")
    publish_log(3)
    got_gain.wait()
    got_wo.wait()
    spread(2)
    spread_twin(2)
    finish_seq(0)
    spread(3, "mid")
    spread_twin(3, "mid")
    spread(3, "end")
    spread_twin(3, "end")
    finish_seq(1, "mid")
    finish_seq(1, "end")
    for j in range(logs.shape[0]):
        for h in range(heads):
            log_out[j, h : h + 1] = logs[j, h]
    while sent:
        drain()


def layer(nsp, ntp, tokens, wq, wk, wv, wo, tables, gain):
    seqs, length, width = tokens.shape
    half = seqs // 2
    cols = wq.shape[1]
    heads = cols // HEAD_DIM
    block = 2 * length
    wide = REACH * FAR
    span = block + 2 * wide
    rows = block // FAR
    near_rows = rows + 2 * FAR
    per = FAR // NEAR
    grans = block // GRAN
    tail = wide - block
    hbm = pl.BlockSpec(memory_space=pl.ANY)
    vmem = pl.BlockSpec(memory_space=pltpu.VMEM)
    v = pltpu.VMEM
    shapes = [((seqs, length, wo.shape[1]), BF16), ((seqs, heads, length), F32)]
    made = pl.pallas_call(
        functools.partial(layer_kernel, nsp),
        in_specs=[hbm] * 10,
        out_specs=[vmem, vmem],
        out_shape=[v(*shape) for shape in shapes],
        scratch_shapes=[
            v(tokens.shape, BF16), v(wq.shape, BF16), v((wk.shape[0], 2 * cols), BF16),
            v(wo.shape, BF16), v((length, HEAD_DIM), F32), v((length, HEAD_DIM), F32),
            v((nsp, HEAD_DIM), F32), v((nsp, HEAD_DIM), F32), v(gain.shape, F32),
            v((half * heads, span, 2 * HEAD_DIM), BF16),
            v((half * heads, block, HEAD_DIM), BF16),
            v((half * heads, length, 2 * HEAD_DIM), BF16),
            v((half * heads, length, HEAD_DIM), BF16),
            v((ntp, seqs, heads, length, HEAD_DIM), BF16),
            v((half * heads, length, HEAD_DIM), BF16),
            v((seqs, heads, 1, length), F32),
            v((half * heads, 1, length), F32),
            v((2, 1, block), F32),
            v((2, FAR, (span - 2 * tail) // FAR, 3 * HEAD_DIM), BF16),
            v((2, FAR, rows, HEAD_DIM), BF16),
            v((2, block, HEAD_DIM), BF16),
            v((GRAN, GRAN), BF16), v((GRAN, GRAN), BF16),
            v((grans, GRAN, GRAN + 2 * REACH), F32),
            v((per * rows, per * near_rows), F32),
            v((rows, (span - 2 * tail) // FAR), F32),
            v((2 * (tail // GRAN), GRAN, tail), F32),
            v((2, FAR, rows, HEAD_DIM), F32),
            v((2, FAR, rows, HEAD_DIM), F32),
            v((2, FAR, rows, HEAD_DIM), F32),
            pltpu.SemaphoreType.DMA((seqs + 12,)),
            pltpu.SemaphoreType.DMA((6 * half * heads,)),
            pltpu.SemaphoreType.DMA((17 * half * heads + 1,)),
        ],
        compiler_params=pltpu.CompilerParams(
            collective_id=0, has_side_effects=True, vmem_limit_bytes=52 * 2**20
        ),
        name="layer",
    )(*(
        pltpu.with_memory_space_constraint(a, pltpu.HBM)
        for a in (tokens, wq, wk, wv, wo, *tables, gain)
    ))
    return pl.pallas_call(
        emit_kernel,
        in_specs=[vmem, vmem],
        out_specs=[hbm, hbm],
        out_shape=[jax.ShapeDtypeStruct(*shape) for shape in shapes],
        scratch_shapes=[pltpu.SemaphoreType.DMA((seqs + 1,))],
        name="emit",
    )(*(pltpu.with_memory_space_constraint(a, v) for a in made))


def emit_kernel(mixed, logs, mixed_h, logs_h, sems):
    pairs = [(mixed.at[j], mixed_h.at[j]) for j in range(mixed.shape[0])] + [(logs, logs_h)]
    copies = [pltpu.make_async_copy(*pair, sems.at[n]) for n, pair in enumerate(pairs)]
    for c in copies:
        c.start()
    for c in copies:
        c.wait()


def shards(tokens, query_weight, key_weight, value_weight, out_gain, out_weight):
    length = tokens.shape[1]
    nsp = lax.axis_size("sp")
    frequency = ROPE_BASE ** (-np.arange(HEAD_DIM // 2) / (HEAD_DIM // 2))
    frequency = np.tile(frequency, 2)[None, :]
    step = np.arange(length)[:, None] * frequency
    base = (np.arange(nsp) * length)[:, None] * frequency
    tables = [
        jnp.asarray(f(a).astype(np.float32)) for a in (step, base) for f in (np.cos, np.sin)
    ]
    return tuple(
        layer(
            nsp, lax.axis_size("tp"), tokens, query_weight, key_weight, value_weight,
            out_weight, tables, out_gain[None, :],
        )
    )


def solution(mesh):
    return jax.shard_map(
        shards,
        mesh=mesh,
        in_specs=(
            P(None, "sp", None),
            P(None, "tp"),
            P(None, "tp"),
            P(None, "tp"),
            P(),
            P(None, "tp"),
        ),
        out_specs=(P(None, "sp", "tp"), P(None, "tp", "sp")),
        check_vma=False,
    )
```

```python
import functools
import math

import jax
import jax.numpy as jnp
import numpy as np
from jax import lax
from jax.experimental import pallas as pl
from jax.experimental.pallas import tpu as pltpu
from jax.sharding import PartitionSpec as P

HEAD_DIM = 128
REACH = 64
FAR = 16
NEAR = 4
GRAN = FAR * FAR
ROPE_BASE = 10000.0
MASK_FILL = -1e30
NORM_FLOOR = 1e-06
LOG2E = 1.0 / math.log(2.0)
LN2 = math.log(2.0)
F32 = jnp.float32
BF16 = jnp.bfloat16

MESH = pl.DeviceIdType.MESH


def iota(shape, dim):
    return lax.broadcasted_iota(jnp.int32, shape, dim)


def perm_token(p):
    slot = p // FAR
    a = p % FAR
    residue = slot // NEAR + NEAR * (slot % (FAR // NEAR))
    return a * FAR + residue


def dot_t(a, b):
    return lax.dot_general(a, b, (((1,), (1,)), ((), ())), preferred_element_type=F32)


def layer_kernel(
    nsp, tok_h, wq_h, wk_h, wv_h, wo_h, cos_h, sin_h, cos_base_h, sin_base_h, gain_h,
    out, log_out,
    tok, wq, wkv, wo, cos, sin, cos_base, sin_base, gain, kn, qn, kvs, qs, gath, outs, logs,
    lsend, lrow, kp, qp, on, perm, unperm, bias1, bias4, bias16, bias_end, o1, m1, l1,
    load_sem, send_sem, recv_sem,
):
    half = tok.shape[0] // 2
    units = kn.shape[0]
    length = tok.shape[1]
    block = 2 * length
    grans = block // GRAN
    wide = REACH * FAR
    side = wide // GRAN
    tail = wide - block
    span = block + 2 * wide
    rows = block // FAR
    ends = tail // GRAN
    key_rows = (span - 2 * tail) // FAR
    near_rows = rows + 2 * FAR
    cols = wq.shape[1]
    heads = cols // HEAD_DIM
    total = nsp * length
    scale = HEAD_DIM**-0.5 * LOG2E
    sp, t = lax.axis_index("sp"), lax.axis_index("tp")
    y, blk = sp % 2, sp // 2
    twin = sp + 1 - 2 * y
    x_peer = (t + 2) % 4
    d_peer = t + 1 - 2 * (t % 2)
    x_d_peer = (d_peer + 2) % 4
    mine, other = y * half, (1 - y) * half

    def lanes(n):
        return slice(n * HEAD_DIM, (n + 1) * HEAD_DIM)

    loads, landed = [], []

    def load(src, dst):
        n = landed.pop(0) if landed else len(loads)
        copy = pltpu.make_async_copy(src, dst, load_sem.at[n])
        copy.start()
        if n == len(loads):
            loads.append(copy)
        return copy

    def land(copies):
        for c in copies:
            c.wait()
            landed.append(next(n for n, one in enumerate(loads) if one is c))

    cuts = (pl.ds(0, length // 3), pl.ds(length // 3, length - length // 3))
    got_first = [load(tok_h.at[mine, cuts[0]], tok.at[0, cuts[0]])]

    def load_kv(h):
        cut = lanes(h)
        got = [load(wk_h.at[:, cut], wkv.at[:, lanes(2 * h)])]
        return [*got, load(wv_h.at[:, cut], wkv.at[:, lanes(2 * h + 1)])]

    got_kv = [load_kv(0)]
    got_tables = [
        load(*pair)
        for pair in (
            (cos_base_h, cos_base), (sin_base_h, sin_base),
            (cos_h.at[cuts[0]], cos.at[cuts[0]]), (sin_h.at[cuts[0]], sin.at[cuts[0]]),
        )
    ]
    got_kv += [load_kv(h) for h in range(1, heads)]
    got_tok = {}

    barrier = pltpu.get_barrier_semaphore()
    has = {d: (sp + d >= 0) & (sp + d < nsp) for d in (2, -2, 4, -4)}
    reach = {d: has[d] & has[-d] for d in (2, -2)}
    beside = ((twin, t), (sp, x_peer), (sp, d_peer), (twin, x_peer))
    for peer in beside:
        pl.semaphore_signal(barrier, inc=1, device_id=peer, device_id_type=MESH)
    count = len(beside)
    for d in (2, -2):
        there = has[d]
        count = count + there.astype(jnp.int32)

        @pl.when(there)
        def _(d=d):
            pl.semaphore_signal(barrier, inc=1, device_id=(sp + d, t), device_id_type=MESH)

    first = pl.multiple_of(y * length, HEAD_DIM)
    second = pl.multiple_of((1 - y) * length, HEAD_DIM)

    def clear(d, at, size):
        @pl.when(jnp.logical_not(has[d]))
        def _():
            for u in range(units):
                kn[u, at : at + size] = jnp.zeros((size, kn.shape[2]), BF16)

    numbers, lane, sent = {}, [0], []

    def copy(name, src, dst, peer):
        n = numbers.setdefault(name, len(numbers))
        return pltpu.make_async_remote_copy(
            src_ref=src, dst_ref=dst, send_sem=send_sem.at[lane[0]], recv_sem=recv_sem.at[n],
            device_id=peer, device_id_type=MESH,
        )

    def when(there, act):
        act() if there is None else pl.when(there)(act)

    def drain():
        c, there, held = sent.pop(0)
        when(there, c.wait_send)
        return held

    def start(make, there=None):
        lane[0] = len(sent) if len(sent) < send_sem.shape[0] else drain()
        c = make()
        when(there, c.start)
        sent.append((c, there, lane[0]))

    opening = [(h, cuts[0]) for h in range(heads)] + [(pl.ds(0, heads), cuts[1])]

    def z_copy(kind, u, d, n=None):
        pick = u
        if kind == "T":
            src = wide - tail if d > 0 else wide + block
            dst = 0 if d > 0 else span - tail
            size = tail
        else:
            if kind == "S":
                at, size = block - tail if d > 0 else 0, tail
            elif kind == "R":
                at, size = 0 if d > 0 else tail, block - tail
            else:
                at, size = first if kind == "A" else second, length
            if n is not None:
                pick, cut = opening[n]
                at, size = at + cut.start, cut.size
            src = wide + at
            dst = (tail if d > 0 else wide + block) + at
        return copy(
            (kind, u, d, n), kn.at[pick, pl.ds(src, size)], kn.at[pick, pl.ds(dst, size)], (sp + d, t)
        )

    def z_start(kind, u, n=None, also=True):
        for d in (2, -2):
            start(lambda: z_copy(kind, u, d, n), also & (reach[d] if kind == "T" else has[d]))

    def z_wait(kind, u):
        for d in (2, -2):

            @pl.when(has[-2 * d] if kind == "T" else has[-d])
            def _():
                for n in range(len(opening)) if kind == "A" and u == 0 else (None,):
                    z_copy(kind, u, d, n).wait_recv()

    every = pl.ds(0, length)

    def rotated(one, cut):
        other_half = pltpu.roll(one, HEAD_DIM // 2, 1)
        return (one * cos[cut] + other_half * sin[cut]).astype(BF16)

    def turned(x, w, store):
        a = jnp.dot(x, w[...], preferred_element_type=F32)
        for h in range(heads):
            store(h, rotated(a[:, lanes(h)], every))

    def keys_values(x, put, cut=every, of_heads=range(heads)):
        for h in of_heads:
            a = jnp.dot(
                x, wkv[:, 2 * h * HEAD_DIM : (2 * h + 2) * HEAD_DIM], preferred_element_type=F32
            )
            put(2 * h, rotated(a[:, :HEAD_DIM], cut))
            put(2 * h + 1, a[:, HEAD_DIM:].astype(BF16))

    def own_kv(s, cut=every, of_heads=range(heads)):
        def put(n, a):
            at = pl.ds(wide + first + cut.start, cut.size)
            kn[s * heads + n // 2, at, lanes(n % 2)] = a

        keys_values(tok[2 * s, cut], put, cut, of_heads)

    def twin_kv(s):
        def put(n, a):
            kvs[s * heads + n // 2, :, lanes(n % 2)] = a

        keys_values(tok[2 * s + 1], put)

    def own_q(s):
        def put(n, a):
            qn[s * heads + n, pl.ds(first, length)] = a

        turned(tok[2 * s], wq, put)

    def twin_q(s):
        def put(n, a):
            qs[s * heads + n] = a

        turned(tok[2 * s + 1], wq, put)

    def y_kv(u, at):
        return copy(("yk", u), kvs.at[u], kn.at[u, pl.ds(wide + at, length)], (twin, t))

    def y_q(s, at):
        pick = pl.ds(s * heads, heads)
        return copy(("yq", s), qs.at[pick], qn.at[pick, pl.ds(at, length)], (twin, t))

    def of(s):
        return range(s * heads, (s + 1) * heads)

    land(got_tables)
    got_rest = [load(a.at[cuts[1]], b.at[cuts[1]]) for a, b in ((cos_h, cos), (sin_h, sin))]
    cos_at, sin_at = cos_base[pl.ds(sp, 1)], sin_base[pl.ds(sp, 1)]

    def angles(cut):
        sign = jnp.where(iota((cut.size, HEAD_DIM), 1) < HEAD_DIM // 2, -1.0, 1.0)
        cos_step, sin_step = cos[cut], sin[cut]
        cos[cut] = cos_step * cos_at - sin_step * sin_at
        sin[cut] = (sin_step * cos_at + cos_step * sin_at) * sign

    angles(cuts[0])
    land(got_first)
    for h in range(heads):
        land(got_kv[h])
        if h == 0:
            got_first.append(load(tok_h.at[mine, cuts[1]], tok.at[0, cuts[1]]))
            got_tok["o", 0] = load(tok_h.at[other], tok.at[1])
        own_kv(0, cuts[0], [h])
        if h == 0:
            pl.semaphore_wait(barrier, count)
        z_start("A", 0, h)
    for c in got_rest:
        c.wait()
    angles(cuts[1])
    got_wq = load(wq_h, wq)
    got_first[1].wait()
    own_kv(0, cuts[1])
    z_start("A", 0, heads)
    got_tok["o", 0].wait()
    for s in range(1, half):
        got_tok["o", s] = load(tok_h.at[other + s], tok.at[2 * s + 1])
        got_tok["m", s] = load(tok_h.at[mine + s], tok.at[2 * s])
    got_gain = load(gain_h, gain)
    got_wo = load(wo_h, wo)
    twin_kv(0)
    for u in of(0):
        start(lambda: y_kv(u, first))
    got_wq.wait()
    twin_q(0)
    start(lambda: y_q(0, first))
    for s in range(1, half):
        got_tok["o", s].wait()
        got_tok["m", s].wait()
        twin_kv(s)
        for u in of(s):
            start(lambda: y_kv(u, first))
        own_kv(s)
        twin_q(s)
        start(lambda: y_q(s, first))
    y_kv(0, second).wait_recv()
    z_start("B", 0)
    own_q(0)

    clear(-4, 0, tail)
    clear(-2, tail, block)
    clear(2, wide + block, block)
    clear(4, span - tail, tail)
    perm[...] = jnp.where(
        iota((GRAN, GRAN), 1) == perm_token(iota((GRAN, GRAN), 0)), 1.0, 0.0
    ).astype(BF16)
    unperm[...] = jnp.where(
        iota((GRAN, GRAN), 0) == perm_token(iota((GRAN, GRAN), 1)), 1.0, 0.0
    ).astype(BF16)
    kp[:, :, :, 2 * HEAD_DIM :] = jnp.ones((*kp.shape[:3], HEAD_DIM), BF16)
    origin = blk * block - wide
    shape = (GRAN, GRAN + 2 * REACH)
    token = perm_token(iota(shape, 0))
    for g in range(grans):
        q_at = wide + g * GRAN + token
        k_at = wide + g * GRAN - REACH + iota(shape, 1)
        ok = (jnp.abs(k_at - q_at) <= REACH) & (k_at + origin >= 0) & (k_at + origin < total)
        bias1[g] = jnp.where(ok, 0.0, MASK_FILL)
    per = FAR // NEAR
    shape = (per * rows, per * near_rows)
    row, col = iota(shape, 0), iota(shape, 1)
    q_at = (row % rows + side * FAR) * FAR + NEAR * (row // rows)
    k_at = (col % near_rows + (side - 1) * FAR) * FAR + NEAR * (col // near_rows)
    ok = (jnp.abs(k_at - q_at) <= REACH * NEAR) & (k_at + origin >= 0) & (k_at + origin < total)
    bias4[...] = jnp.where(ok, 0.0, MASK_FILL)
    shape = (rows, key_rows)
    q_at = iota(shape, 0) + side * FAR
    k_at = iota(shape, 1) + ends * FAR
    ok = (
        (jnp.abs(k_at - q_at) <= REACH)
        & (k_at * FAR + origin >= 0)
        & (k_at * FAR + origin < total)
    )
    bias16[...] = jnp.where(ok, 0.0, MASK_FILL)
    reached = [(0, 0), (grans - 1, span - tail)]
    shape = (GRAN, tail)
    token = perm_token(iota(shape, 0))
    for n, (g, at) in enumerate(reached):
        gap = at + iota(shape, 1) - (wide + g * GRAN + token)
        k_at = at + iota(shape, 1) + origin
        ok = (gap % FAR == 0) & (jnp.abs(gap) <= wide) & (k_at >= 0) & (k_at < total)
        bias_end[n] = jnp.where(ok, 0.0, MASK_FILL)

    y_kv(1, second).wait_recv()
    z_start("B", 1)
    for s in range(1, half):
        own_q(s)

    near_from, near_to = side - 1, side + grans + 1

    def gather_keys(u, slot, chunks):
        for j in chunks:
            moved = jnp.dot(
                perm[...], kn[u, j * GRAN : (j + 1) * GRAN], preferred_element_type=F32
            )
            moved = moved.astype(BF16).reshape(FAR, FAR, 2 * HEAD_DIM)
            at = (j - ends) * FAR
            kp[slot, :, at : at + FAR, : 2 * HEAD_DIM] = moved

    flat = (per * rows, HEAD_DIM)
    cube = (per, rows, HEAD_DIM)

    def merge(slot, sel, scores, weigh):
        m_old = m1[slot, sel].reshape(flat)
        m_new = jnp.maximum(m_old, jnp.max(scores, axis=1, keepdims=True))
        keep = jnp.exp2(m_old - m_new)
        p = jnp.exp2(scores - m_new[:, :1])
        o_l = weigh(p.astype(BF16))
        l = l1[slot, sel].reshape(flat) * keep + o_l[:, HEAD_DIM:]
        o = o1[slot, sel].reshape(flat) * keep + o_l[:, :HEAD_DIM]
        for ref, a in ((o1, o), (m1, m_new), (l1, l)):
            ref[slot, sel] = a.reshape(cube)

    def with_ones(v):
        return jnp.concatenate([v, jnp.ones_like(v)], axis=1)

    def attend_near(u):
        slot = u % 2
        if u % heads == 0:
            y_q(u // heads, second).wait_recv()
        gather_keys(u, slot, range(near_from, near_to))
        for g in range(grans):
            moved = jnp.dot(
                perm[...], qn[u, g * GRAN : (g + 1) * GRAN], preferred_element_type=F32
            )
            moved = moved.astype(BF16)
            qp[slot, :, g * FAR : (g + 1) * FAR] = moved.reshape(FAR, FAR, HEAD_DIM)
            at = wide + g * GRAN - REACH
            k = kn[u, at : at + GRAN + 2 * REACH, :HEAD_DIM]
            v = with_ones(kn[u, at : at + GRAN + 2 * REACH, HEAD_DIM:])
            sc = dot_t(moved, k) * scale + bias1[g]
            m = jnp.max(sc, axis=1, keepdims=True)
            p = jnp.exp2(sc - m)
            o_l = jnp.dot(p.astype(BF16), v, preferred_element_type=F32)
            o, l = o_l[:, :HEAD_DIM], o_l[:, HEAD_DIM:]
            for ref, a in ((o1, o), (m1, jnp.broadcast_to(m, o.shape)), (l1, l)):
                ref[slot, :, g * FAR : (g + 1) * FAR] = a.reshape(FAR, FAR, HEAD_DIM)

        near_at = (near_from - ends) * FAR
        for group in range(NEAR):
            sel = slice(group * per, (group + 1) * per)
            k4 = kp[slot, sel, near_at : near_at + near_rows, :HEAD_DIM].reshape(-1, HEAD_DIM)
            v4 = kp[slot, sel, near_at : near_at + near_rows, HEAD_DIM:].reshape(-1, 2 * HEAD_DIM)
            s4 = dot_t(qp[slot, sel].reshape(flat), k4) * scale + bias4[...]
            merge(slot, sel, s4, lambda p: jnp.dot(p, v4, preferred_element_type=F32))

    def attend_far(u):
        slot = u % 2
        gather_keys(u, slot, [*range(ends, near_from), *range(near_to, span // GRAN - ends)])
        for group in range(NEAR):
            sel = slice(group * per, (group + 1) * per)
            own = range(group * per, (group + 1) * per)
            b16 = bias16[...]
            s16 = [dot_t(qp[slot, r], kp[slot, r, :, :HEAD_DIM]) * scale + b16 for r in own]

            def weigh(p):
                return jnp.concatenate(
                    [
                        jnp.dot(
                            p[i * rows : (i + 1) * rows], kp[slot, r, :, HEAD_DIM:],
                            preferred_element_type=F32,
                        )
                        for i, r in enumerate(own)
                    ],
                    axis=0,
                )

            merge(slot, sel, jnp.concatenate(s16, axis=0), weigh)
        for g in range(ends, grans - ends):
            o, _, l = state(slot, g)
            settle(slot, g, o, l)

    def slots_of(g):
        return pl.ds(g * FAR, FAR)

    def state(slot, g):
        cut = slots_of(g)
        return [ref[slot, :, cut].reshape(GRAN, HEAD_DIM) for ref in (o1, m1, l1)]

    def settle(slot, g, o, l):
        merged = jnp.dot(unperm[...], (o / l).astype(BF16), preferred_element_type=F32)
        on[slot, pl.ds(g * GRAN, GRAN)] = merged.astype(BF16)

    def settle_log(slot, g):
        _, m, l = state(slot, g)
        x = m * LN2 + jnp.log(l)
        high = x.astype(BF16).astype(F32)
        mid = (x - high).astype(BF16).astype(F32)
        low = x - high - mid
        lane_at = iota((GRAN, HEAD_DIM), 1)
        terms = jnp.where(
            lane_at == 0, high, jnp.where(lane_at == 1, mid, jnp.where(lane_at == 2, low, 0.0))
        )
        pick = jnp.where(iota((FAR, HEAD_DIM), 0) == iota((FAR, HEAD_DIM), 1), 1.0, 0.0)
        turned_terms = dot_t(pick.astype(BF16), terms.astype(BF16)).astype(BF16)
        placed = jnp.dot(turned_terms, perm[...], preferred_element_type=F32)
        lrow[slot, :, g * GRAN : (g + 1) * GRAN] = jnp.sum(placed, axis=0, keepdims=True)

    def attend_side(u, n):
        slot = u % 2
        g, at = n * (grans - 1), n * (span - tail)
        if not isinstance(n, int):
            at = pl.multiple_of(at, GRAN)
        cut = slots_of(g)
        o_old, m_old, l_old = state(slot, g)
        q = qp[slot, :, cut].reshape(GRAN, HEAD_DIM)
        k = kn[u, pl.ds(at, tail), :HEAD_DIM]
        v = with_ones(kn[u, pl.ds(at, tail), HEAD_DIM:])
        sc = dot_t(q, k) * scale + bias_end[n]
        m = jnp.maximum(m_old, jnp.max(sc, axis=1, keepdims=True))
        keep = jnp.exp2(m_old - m)
        p = jnp.exp2(sc - m[:, :1])
        o_l = jnp.dot(p.astype(BF16), v, preferred_element_type=F32)
        l = l_old * keep + o_l[:, HEAD_DIM:]
        settle(slot, g, o_old * keep + o_l[:, :HEAD_DIM], l)
        m1[slot, :, cut] = m.reshape(FAR, FAR, HEAD_DIM)
        l1[slot, :, cut] = l.reshape(FAR, FAR, HEAD_DIM)

    def attend_end(u):
        z_wait("T", u)
        for n in range(len(reached)):
            attend_side(u, n)

    def some(part, half_at):
        if part is None:
            return every
        at = (1 - half_at) * tail if part == "mid" else half_at * (length - tail)
        size = length - tail if part == "mid" else tail
        return pl.ds(pl.multiple_of(at, HEAD_DIM), size)

    def across(u, base, half_at, part):
        cut = some(part, half_at)
        return copy(
            ("yo", u, part), outs.at[u, cut], gath.at[t, base + u // heads, u % heads, cut],
            (twin, t),
        )

    def log_across(s, base):
        return copy(("yl", s), lsend.at[pl.ds(s * heads, heads)], logs.at[base + s], (twin, t))

    def corner(u, part):
        cut = some(part, 1 - y)
        return copy(
            ("xr", u, part), outs.at[u, cut],
            gath.at[t, mine + u // heads, u % heads, cut], (twin, x_peer),
        )

    def piece(name, u, owner, base, peer, part):
        ref = gath.at[owner, base + u // heads, u % heads, some(part, y)]
        return copy((name, u, part), ref, ref, peer)

    def put(u, ref, half_at, part):
        cut = some(part, half_at)
        at = pl.multiple_of(half_at * length + cut.start, HEAD_DIM)
        ref[cut] = on[u % 2, pl.ds(at, cut.size)]

    def publish_twin(u, part=None):
        put(u, outs.at[u], 1 - y, part)
        start(lambda: corner(u, part))
        start(lambda: across(u, mine, 1 - y, part))

    def publish_own(u, part=None):
        s, h = u // heads, u % heads
        put(u, gath.at[t, mine + s, h], y, part)
        start(lambda: piece("xm", u, t, mine, (sp, x_peer), part))
        start(lambda: piece("dm", u, t, mine, (sp, d_peer), part))

    def publish_log(u):
        slot = u % 2
        s, h = u // heads, u % heads
        for g in range(grans):
            settle_log(slot, g)
        logs[mine + s, h] = lrow[slot, :, pl.ds(first, length)]
        lsend[u] = lrow[slot, :, pl.ds(second, length)]
        if h == heads - 1:
            start(lambda: log_across(s, mine))

    def publish(u):
        publish_twin(u)
        publish_own(u)
        publish_log(u)

    def spread(u, part=None):
        across(u, other, y, part).wait_recv()
        start(lambda: piece("dr", u, t, other, (sp, d_peer), part))
        piece("xm", u, x_peer, mine, (sp, x_peer), part).wait_recv()
        start(lambda: piece("em", u, x_peer, mine, (sp, d_peer), part))

    def spread_twin(u, part=None):
        piece("xr", u, x_peer, other, (sp, x_peer), part).wait_recv()
        start(lambda: piece("er", u, x_peer, other, (sp, d_peer), part))
        if part != "mid" and u % heads == heads - 1:
            log_across(u // heads, other).wait_recv()

    def finish(js, cut):
        acc = None
        squares = None
        for n in range(gath.shape[0]):
            xs = [
                jnp.concatenate([gath[n, j, h, cut] for j in js], axis=0).astype(F32)
                for h in range(heads)
            ]
            at = slice(n * cols, (n + 1) * cols)
            scaled = (jnp.concatenate(xs, axis=1) * gain[:, at]).astype(BF16)
            term = jnp.dot(scaled, wo[at], preferred_element_type=F32)
            acc = term if acc is None else acc + term
            for x in xs:
                squares = x * x if squares is None else squares + x * x
        square = jnp.sum(squares, axis=1, keepdims=True)
        a = (acc * lax.rsqrt(square / wo.shape[0] + NORM_FLOOR)).astype(BF16)
        for n, j in enumerate(js):
            out[j, cut] = a[n * cut.size : (n + 1) * cut.size]

    def finish_seq(s, part=None):
        for kinds, base in ((("dm", "em"), mine), (("dr", "er"), other)):
            for u in of(s):
                for p in parts_of(u, part):
                    for kind, owner in zip(kinds, (d_peer, x_d_peer)):
                        piece(kind, u, owner, base, (sp, d_peer), p).wait_recv()
        finish((mine + s, other + s), some(part, y))

    def parts_of(u, part):
        if u == units - 1:
            return (part,)
        return () if part == "end" else (None,)

    def arrived(u):
        if u == 0 or u >= heads:
            z_wait("A", u)
        z_wait("B", u)

    arrived(0)
    z_start("T", 0)
    z_start("A", 2)
    attend_near(0)
    attend_far(0)
    arrived(1)
    z_start("T", 1)
    attend_near(1)
    y_kv(2, second).wait_recv()
    z_start("B", 2)
    attend_end(0)
    publish(0)
    attend_far(1)
    y_kv(3, second).wait_recv()
    z_start("S", 3)
    attend_end(1)
    publish(1)
    arrived(2)
    z_start("T", 2)
    z_start("R", 3)
    attend_near(2)
    attend_far(2)
    z_wait("S", 3)
    z_start("T", 3, also=t % 2 == 0)
    attend_near(3)
    attend_end(2)
    publish(2)
    spread(0)
    spread_twin(0)
    spread(1)
    spread_twin(1)
    z_wait("R", 3)
    z_start("T", 3, also=t % 2 == 1)
    attend_far(3)
    publish_twin(3, "mid")
    publish_own(3, "mid")
    z_wait("T", 3)
    attend_side(3, 1 - y)
    publish_twin(3, "end")
    attend_side(3, y)
    publish_own(3, "end")
    publish_log(3)
    got_gain.wait()
    got_wo.wait()
    spread(2)
    spread_twin(2)
    finish_seq(0)
    spread(3, "mid")
    spread_twin(3, "mid")
    spread(3, "end")
    spread_twin(3, "end")
    finish_seq(1, "mid")
    finish_seq(1, "end")
    for j in range(logs.shape[0]):
        for h in range(heads):
            log_out[j, h : h + 1] = logs[j, h]
    while sent:
        drain()


def layer(nsp, ntp, tokens, wq, wk, wv, wo, tables, gain):
    seqs, length, width = tokens.shape
    half = seqs // 2
    cols = wq.shape[1]
    heads = cols // HEAD_DIM
    block = 2 * length
    wide = REACH * FAR
    span = block + 2 * wide
    rows = block // FAR
    near_rows = rows + 2 * FAR
    per = FAR // NEAR
    grans = block // GRAN
    tail = wide - block
    hbm = pl.BlockSpec(memory_space=pl.ANY)
    vmem = pl.BlockSpec(memory_space=pltpu.VMEM)
    v = pltpu.VMEM
    shapes = [((seqs, length, wo.shape[1]), BF16), ((seqs, heads, length), F32)]
    made = pl.pallas_call(
        functools.partial(layer_kernel, nsp),
        in_specs=[hbm] * 10,
        out_specs=[vmem, vmem],
        out_shape=[v(*shape) for shape in shapes],
        scratch_shapes=[
            v(tokens.shape, BF16), v(wq.shape, BF16), v((wk.shape[0], 2 * cols), BF16),
            v(wo.shape, BF16), v((length, HEAD_DIM), F32), v((length, HEAD_DIM), F32),
            v((nsp, HEAD_DIM), F32), v((nsp, HEAD_DIM), F32), v(gain.shape, F32),
            v((half * heads, span, 2 * HEAD_DIM), BF16),
            v((half * heads, block, HEAD_DIM), BF16),
            v((half * heads, length, 2 * HEAD_DIM), BF16),
            v((half * heads, length, HEAD_DIM), BF16),
            v((ntp, seqs, heads, length, HEAD_DIM), BF16),
            v((half * heads, length, HEAD_DIM), BF16),
            v((seqs, heads, 1, length), F32),
            v((half * heads, 1, length), F32),
            v((2, 1, block), F32),
            v((2, FAR, (span - 2 * tail) // FAR, 3 * HEAD_DIM), BF16),
            v((2, FAR, rows, HEAD_DIM), BF16),
            v((2, block, HEAD_DIM), BF16),
            v((GRAN, GRAN), BF16), v((GRAN, GRAN), BF16),
            v((grans, GRAN, GRAN + 2 * REACH), F32),
            v((per * rows, per * near_rows), F32),
            v((rows, (span - 2 * tail) // FAR), F32),
            v((2 * (tail // GRAN), GRAN, tail), F32),
            v((2, FAR, rows, HEAD_DIM), F32),
            v((2, FAR, rows, HEAD_DIM), F32),
            v((2, FAR, rows, HEAD_DIM), F32),
            pltpu.SemaphoreType.DMA((seqs + 2 * heads + 1,)),
            pltpu.SemaphoreType.DMA((6 * half * heads,)),
            pltpu.SemaphoreType.DMA((17 * half * heads + 1,)),
        ],
        compiler_params=pltpu.CompilerParams(
            collective_id=0, has_side_effects=True, vmem_limit_bytes=52 * 2**20
        ),
        name="layer",
    )(*(
        pltpu.with_memory_space_constraint(a, pltpu.HBM)
        for a in (tokens, wq, wk, wv, wo, *tables, gain)
    ))
    return pl.pallas_call(
        emit_kernel,
        in_specs=[vmem, vmem],
        out_specs=[hbm, hbm],
        out_shape=[jax.ShapeDtypeStruct(*shape) for shape in shapes],
        scratch_shapes=[pltpu.SemaphoreType.DMA((seqs + 1,))],
        name="emit",
    )(*(pltpu.with_memory_space_constraint(a, v) for a in made))


def emit_kernel(mixed, logs, mixed_h, logs_h, sems):
    pairs = [(mixed.at[j], mixed_h.at[j]) for j in range(mixed.shape[0])] + [(logs, logs_h)]
    copies = [pltpu.make_async_copy(*pair, sems.at[n]) for n, pair in enumerate(pairs)]
    for c in copies:
        c.start()
    for c in copies:
        c.wait()


def shards(tokens, query_weight, key_weight, value_weight, out_gain, out_weight):
    length = tokens.shape[1]
    nsp = lax.axis_size("sp")
    frequency = ROPE_BASE ** (-np.arange(HEAD_DIM // 2) / (HEAD_DIM // 2))
    frequency = np.tile(frequency, 2)[None, :]
    step = np.arange(length)[:, None] * frequency
    base = (np.arange(nsp) * length)[:, None] * frequency
    tables = [
        jnp.asarray(f(a).astype(np.float32)) for a in (step, base) for f in (np.cos, np.sin)
    ]
    return tuple(
        layer(
            nsp, lax.axis_size("tp"), tokens, query_weight, key_weight, value_weight,
            out_weight, tables, out_gain[None, :],
        )
    )


def solution(mesh):
    return jax.shard_map(
        shards,
        mesh=mesh,
        in_specs=(
            P(None, "sp", None),
            P(None, "tp"),
            P(None, "tp"),
            P(None, "tp"),
            P(),
            P(None, "tp"),
        ),
        out_specs=(P(None, "sp", "tp"), P(None, "tp", "sp")),
        check_vma=False,
    )
```
